32 devices in a mesh: sp: 16 (over z, y, x), tp: 2 (over core).
Axes of the slice: x: 2, y: 2, z: 4, core: 2. Of those that a mesh axis runs over, the one named last changes fastest.
Arguments:
- resid: bfloat16 [2048, 2048], P(('sp', 'tp')), may hold values from -3 to 3
- queries: bfloat16 [2048, 2048], P('sp', 'tp'), may hold values from -6 to 6
- keys: bfloat16 [2048, 2048], P('sp', 'tp'), may hold values from -6 to 6
- values: bfloat16 [2048, 2048], P('sp', 'tp'), may hold values from -8 to 8
- doc_ids: int32 [2048], P('sp'), may hold values from 0 to 3, never falling along the last dimension, each value on 1 to 896 neighbouring positions
- score_offset: float32 [32], P('tp'), may hold values from -10 to -3
- out_weight: bfloat16 [2048, 2048], P('tp'), may hold values from -0.1875 to 0.1875
- norm_gain: float32 [2048], replicated, may hold values from 0.1 to 1.9
- gate_weight: bfloat16 [2048, 6144], P('sp', 'tp'), may hold values from -0.125 to 0.125
- up_weight: bfloat16 [2048, 6144], P('sp', 'tp'), may hold values from -0.125 to 0.125
- down_weight: bfloat16 [6144, 2048], P('tp', 'sp'), may hold values from -0.078125 to 0.078125
Outputs:
- layer_out: bfloat16 [2048, 2048], P(('sp', 'tp'))
The draws below stay inside these ranges and needn't reach their ends.
Inputs may be any that keep to these rules, and one draw needn't show every extreme that they name: `doc_ids`: document numbers never fall along the sequence; each document has 1 to 896 positions, and one has exactly 896.
All inputs are finite; a program needn't handle non-finite values.
Results may differ from the reference program's by a relative error of at most 0.017.
Values may be sent and summed in bfloat16 or wider, within the bound.
A program may use at most 128 MiB of HBM per device.

```python
import math
import jax
import jax.numpy as jnp
import numpy as np
from jax import lax

D = 2048
HEADS = 32
HEAD_DIM = 64
FF = 6144
TOK_DEV = 128
TOKENS = 2048
DOCS = 4
DOC_MOST = 896
N_TP = 2


def draw_score_offset(key, part):
    pick_key = jax.random.fold_in(key, 11)
    slow_key = jax.random.fold_in(key, 12)
    fast_key = jax.random.fold_in(key, 13)
    quick = jax.random.bernoulli(pick_key, 0.5, (HEADS,))
    rate = jax.random.uniform(slow_key, (HEADS,), jnp.float32, 0.5, 2.5)
    slow_offset = jnp.log(rate / DOC_MOST) - 0.5
    fast_offset = jnp.log(jax.random.uniform(fast_key, (HEADS,), jnp.float32, 1.0 / 80.0, 1.0 / 30.0)) - 0.5
    return jnp.clip(jnp.where(quick, fast_offset, slow_offset), -10.0, -3.0).astype(jnp.float32)


def draw_values(key, part):
    span_key = jax.random.fold_in(key, 21)
    noise_key = jax.random.fold_in(key, 22)
    width = HEADS * HEAD_DIM
    spans = TOKENS // TOK_DEV
    common = jax.random.normal(span_key, (spans, 1, width), jnp.float32)
    noise = 0.5 * jax.random.normal(noise_key, (spans, TOK_DEV, width), jnp.float32)
    return jnp.clip(common + noise, -8.0, 8.0).reshape(TOKENS, width).astype(jnp.bfloat16)


def shard_levels(own_key, dims, split, smallest, top_value):
    def one(position, shards_of):
        draws = jax.random.uniform(jax.random.fold_in(jax.random.fold_in(own_key, 6), position), (shards_of,), jnp.float32, smallest / len(split), top_value / len(split))
        return jnp.repeat(jnp.exp(draws), dims[position] // shards_of).reshape((-1,) + (1,) * (len(dims) - position - 1))

    factor_of = one(*split[0])
    for cut in split[1:]:
        factor_of = factor_of * one(*cut)
    return factor_of


def profile(amount, total, reach, slope):
    loads = [(1 << 20) // math.isqrt(grade ** slope) + 1 for grade in range(2, amount + 1)]
    surplus, counts = total - reach - (amount - 1), [1] * (amount - 1)
    while surplus > 0:
        movable = [i for i in range(amount - 1) if counts[i] < reach]
        whole, left = sum([loads[i] for i in movable]), surplus
        for i in movable:
            addition = min(reach - counts[i], max(1, left * loads[i] // whole), surplus)
            counts[i] = counts[i] + addition
            surplus = surplus - addition
    return np.array([reach] + counts)


def uneven_parts(stream_key, number_of, total, bound, skew):
    if number_of == 2:
        one = jax.random.randint(stream_key, (), max(1, total - bound), min(bound, total - 1) + 1)
        return jnp.stack([one, total - one])
    lengths = jnp.asarray(profile(number_of, total, bound, skew), jnp.int32)
    couples = (number_of - 1) // 2
    source_of, taker = lengths[1:1 + 2 * couples:2], lengths[2:2 + 2 * couples:2]
    margin = jnp.minimum(source_of - 1, bound - taker)
    moved = jax.random.randint(jax.random.fold_in(stream_key, 1), (couples,), 0, 1 << 20) % (margin + 1)
    lengths = lengths.at[1:1 + 2 * couples:2].set(source_of - moved).at[2:2 + 2 * couples:2].set(taker + moved)
    return lengths[jax.random.permutation(jax.random.fold_in(stream_key, 2), number_of)]


def gaussian(rng, shape, deviation, most, split=(), held_as=jnp.bfloat16):
    entries = jax.random.normal(rng, shape, jnp.float32) * deviation
    if len(split) > 0:
        entries = shard_levels(rng, shape, split, -0.22, 0.18) * entries
    return jnp.clip(entries, min=-most, max=most).astype(held_as)


def setup_inputs(seed: int = 0) -> dict:
    seeds = jax.random.split(jax.random.key(seed), 12)
    resid = gaussian(seeds[0], (TOKENS, D), 0.5, 3.0, ((0, 32),))
    queries = gaussian(seeds[1], (TOKENS, HEADS * HEAD_DIM), 1.0, 6.0, ((0, 16), (1, 2)))
    keys = gaussian(seeds[2], (TOKENS, HEADS * HEAD_DIM), 1.0, 6.0, ((0, 16), (1, 2)))
    values = draw_values(jax.random.fold_in(seeds[11], 71), 0)
    doc_ids = jnp.searchsorted(jnp.cumsum(uneven_parts(seeds[4], DOCS, TOKENS, DOC_MOST, 1)), jnp.arange(TOKENS), side="right").astype(jnp.int32)
    score_offset = draw_score_offset(jax.random.fold_in(seeds[11], 71), 0)
    out_weight = gaussian(seeds[6], (HEADS * HEAD_DIM, D), (HEADS * HEAD_DIM // 2) ** -0.5, 0.1875, ((0, 2),))
    norm_gain = jnp.clip(1.0 + 0.18 * jax.random.normal(seeds[7], (D,), jnp.float32), 0.1, 1.9)
    gate_weight = gaussian(seeds[8], (D, FF), D ** -0.5, 0.125, ((0, 16), (1, 2)))
    up_weight = gaussian(seeds[9], (D, FF), D ** -0.5, 0.125, ((0, 16), (1, 2)))
    down_weight = gaussian(seeds[10], (FF, D), FF ** -0.5, 0.078125, ((0, 2), (1, 16)))
    return dict(resid=resid, queries=queries, keys=keys, values=values, doc_ids=doc_ids, score_offset=score_offset, out_weight=out_weight, norm_gain=norm_gain, gate_weight=gate_weight, up_weight=up_weight, down_weight=down_weight)


def head_attention(q_head, k_head, v_head, doc_ids, offset):
    q_block = math.gcd(TOKENS, 512)
    extent = min(TOKENS, q_block + DOC_MOST)
    blocks = TOKENS // q_block
    scale = HEAD_DIM ** (-0.5)

    def block(index):
        start = (index * q_block).astype(jnp.int32)
        k_start = jnp.clip(start + q_block - extent, 0, TOKENS - extent).astype(jnp.int32)
        q_rows = lax.dynamic_slice_in_dim(q_head, start, q_block, 0)
        q_docs = lax.dynamic_slice_in_dim(doc_ids, start, q_block, 0)
        k_rows = lax.dynamic_slice_in_dim(k_head, k_start, extent, 0)
        v_rows = lax.dynamic_slice_in_dim(v_head, k_start, extent, 0)
        k_docs = lax.dynamic_slice_in_dim(doc_ids, k_start, extent, 0)
        q_pos = start + jnp.arange(q_block, dtype=jnp.int32)
        key_pos = k_start + jnp.arange(extent, dtype=jnp.int32)
        scores = lax.dot_general(q_rows, k_rows, (((1,), (1,)), ((), ())), preferred_element_type=jnp.float32) * scale + offset
        live = (key_pos[None, :] < q_pos[:, None]) & (k_docs[None, :] == q_docs[:, None])
        log_keep = jnp.where(live, jax.nn.log_sigmoid(-scores), 0.0)
        tail = lax.cumsum(log_keep, axis=1, reverse=True) - log_keep
        weight = jnp.where(live, jnp.exp(jax.nn.log_sigmoid(scores) + tail), 0.0).astype(jnp.bfloat16)
        return jnp.dot(weight, v_rows, preferred_element_type=jnp.float32).astype(jnp.bfloat16)
    result = lax.map(block, jnp.arange(blocks, dtype=jnp.int32))
    return result.reshape(TOKENS, HEAD_DIM)

def reference(resid, queries, keys, values, doc_ids, score_offset, out_weight, norm_gain, gate_weight, up_weight, down_weight):
    heads_out = []
    for head in range(HEADS):
        cols = slice(head * HEAD_DIM, (head + 1) * HEAD_DIM)
        heads_out.append(head_attention(queries[:, cols], keys[:, cols], values[:, cols], doc_ids, score_offset[head]))
    attended = jnp.concatenate(heads_out, axis=1)
    group_width = HEADS // N_TP * HEAD_DIM
    mixed_attn = jnp.zeros((TOKENS, D), jnp.float32)
    for group in range(N_TP):
        cols = slice(group * group_width, (group + 1) * group_width)
        partial_out = jnp.dot(attended[:, cols], out_weight[cols, :], preferred_element_type=jnp.float32)
        mixed_attn = mixed_attn + partial_out.astype(jnp.bfloat16).astype(jnp.float32)
    stream = resid.astype(jnp.float32) + mixed_attn
    normed = (stream * lax.rsqrt(lax.optimization_barrier(jnp.mean(stream * stream, axis=1, keepdims=True)) + 1e-06) * norm_gain).astype(jnp.bfloat16)
    unit_width = FF // N_TP
    feed = jnp.zeros((TOKENS, D), jnp.float32)
    for group in range(N_TP):
        cols = slice(group * unit_width, (group + 1) * unit_width)
        gate = jnp.dot(normed, gate_weight[:, cols], preferred_element_type=jnp.float32)
        upper = jnp.dot(normed, up_weight[:, cols], preferred_element_type=jnp.float32)
        hidden = (jax.nn.silu(gate) * upper).astype(jnp.bfloat16)
        partial_out = jnp.dot(hidden, down_weight[cols, :], preferred_element_type=jnp.float32)
        feed = feed + partial_out.astype(jnp.bfloat16).astype(jnp.float32)
    return (stream + feed).astype(jnp.bfloat16)
```

```python
import functools

import jax
import jax.numpy as jnp
from jax import lax
from jax.experimental import pallas as pl
from jax.experimental.pallas import tpu as pltpu
from jax.sharding import PartitionSpec as P


def from_behind(shard, axis, by):
    peers = lax.axis_size(axis)
    pairs = [(i, i + by) for i in range(peers) if 0 <= i + by < peers]
    return lax.ppermute(shard, axis, pairs)


def as_sent(shard):
    return jax.tree.map(lambda a: a.astype(jnp.bfloat16) if a.dtype == jnp.float32 else a, shard)


def joined(earlier, later):
    return (
        jnp.concatenate([earlier[0], later[0]], axis=0),
        jnp.concatenate([earlier[1], later[1]], axis=0),
        jnp.concatenate([earlier[2], later[2]], axis=0),
    )


def block_update(carry, block, start, context):
    queries_h, q_pos, q_docs, offsets, scale = context
    total, carried = carry
    k_block, v_block, d_block = block
    count = k_block.shape[0]
    heads = offsets.shape[0]
    head_dim = queries_h.shape[2]

    def compute():
        key_pos = start + jnp.arange(count, dtype=jnp.int32)
        live = (
            (key_pos[None, :] >= 0)
            & (key_pos[None, :] < q_pos[:, None])
            & (d_block[None, :] == q_docs[:, None])
        )
        k_heads = k_block.reshape(count, heads, head_dim)
        v_heads = v_block.reshape(count, heads, head_dim)
        scores = (
            jnp.einsum("thd,shd->hts", queries_h, k_heads, preferred_element_type=jnp.float32)
            * scale
            + offsets[:, None, None]
        )
        log_keep = jnp.where(live[None], jax.nn.log_sigmoid(-scores), 0.0)
        tail = lax.cumsum(log_keep, axis=2, reverse=True) - log_keep + carried[:, :, None]
        weight = jnp.where(live[None], jnp.exp(jax.nn.log_sigmoid(scores) + tail), 0.0).astype(
            jnp.bfloat16
        )
        added = jnp.einsum("hts,shd->thd", weight, v_heads, preferred_element_type=jnp.float32)
        return (total + added, carried + jnp.sum(log_keep, axis=2))

    reached = (start + count > 0) & (d_block[-1] >= q_docs[0])
    return lax.cond(reached, compute, lambda: carry)


def windowed(
    resid,
    queries,
    keys,
    values,
    doc_ids,
    score_offset,
    out_weight,
    norm_gain,
    gate_weight,
    up_weight,
    down_weight,
):
    rows = queries.shape[0]
    heads = score_offset.shape[0]
    head_dim = queries.shape[1] // heads
    base = lax.axis_index("sp") * rows
    q_pos = base + jnp.arange(rows, dtype=jnp.int32)
    context = (
        queries.reshape(rows, heads, head_dim),
        q_pos,
        doc_ids,
        score_offset,
        head_dim ** (-0.5),
    )
    own = (keys, values, doc_ids)
    carry = (jnp.zeros((rows, heads, head_dim), jnp.float32), jnp.zeros((heads, rows), jnp.float32))
    nearest = from_behind((keys, values, doc_ids), "sp", 1)
    paired = joined(nearest, own)
    carry = block_update(carry, paired, base - rows, context)
    middle = from_behind((paired[0], paired[1], as_sent(paired[2])), "sp", 2)
    carry = block_update(carry, middle, base - 3 * rows, context)
    fourfold = joined(middle, paired)
    farthest = from_behind((fourfold[0], fourfold[1], as_sent(fourfold[2])), "sp", 4)
    carry = block_update(
        carry, tuple((piece[2 * rows :] for piece in farthest)), base - 5 * rows, context
    )
    carry = block_update(
        carry, tuple((piece[: 2 * rows] for piece in farthest)), base - 7 * rows, context
    )
    attended = carry[0].reshape(rows, heads * head_dim).astype(jnp.bfloat16)
    mixed_attn = lax.psum_scatter(
        jnp.dot(attended, out_weight, preferred_element_type=jnp.float32).astype(jnp.bfloat16),
        "tp",
        scatter_dimension=0,
        tiled=True,
    ).astype(jnp.float32)
    stream = resid.astype(jnp.float32) + mixed_attn
    normed = (
        stream * lax.rsqrt(jnp.mean(stream * stream, axis=1, keepdims=True) + 1e-06) * norm_gain
    ).astype(jnp.bfloat16)
    span_rows = lax.all_gather(normed, "tp", axis=0, tiled=True)
    gate = jnp.dot(
        span_rows,
        lax.all_gather(gate_weight, "sp", axis=0, tiled=True),
        preferred_element_type=jnp.float32,
    )
    upper = jnp.dot(
        span_rows,
        lax.all_gather(up_weight, "sp", axis=0, tiled=True),
        preferred_element_type=jnp.float32,
    )
    hidden = (jax.nn.silu(gate) * upper).astype(jnp.bfloat16)
    partial_out = jnp.dot(
        hidden,
        lax.all_gather(down_weight, "sp", axis=1, tiled=True),
        preferred_element_type=jnp.float32,
    )
    feed = lax.psum_scatter(
        partial_out.astype(jnp.bfloat16), "tp", scatter_dimension=0, tiled=True
    ).astype(jnp.float32)
    return (stream + feed).astype(jnp.bfloat16)


DOC_MOST = 896
LOG2E = 1.4426950408889634
DEAD = -1e30
MESH = pl.DeviceIdType.MESH


def sends(src, dst, send, recv, target):
    return pltpu.make_async_remote_copy(
        src_ref=src, dst_ref=dst, send_sem=send, recv_sem=recv, device_id=target, device_id_type=MESH
    )


def layer_kernel(
    n,
    q_ref, k_ref, v_ref, doc_ref, off_ref, g_in, u_in, d_in, resid_ref, gain_ref, o_in,
    out_ref,
    sbuf, rbuf, docr, ao, att_ref, wg, wu, wd, ow,
    attd, mixed, mixed_in, stream, ag, hid, part, fy, zr,
    qkv_s, qkv_r, doc_s, doc_r, att_s, att_r, w_s, w_r, wx_s, wc_s, own_sem, o_sem, mix_s, mix_r, net_s, net_r,
):
    s = lax.axis_index("sp")
    c = lax.axis_index("tp")
    rows = q_ref.shape[0]
    half = rows // 2
    dim = q_ref.shape[1] // n
    width = wg.shape[1]
    per = g_in.shape[1] // width
    depth = g_in.shape[0]
    dcols = d_in.shape[1]
    levels = n // 4
    back = -(-DOC_MOST // rows)
    other = 1 - c
    x, y, z = lax.rem(s, 2), lax.rem(lax.div(s, 2), 2), lax.div(s, 4)
    g = lax.div(s, 2)
    xn, yn = s + 1 - 2 * x, s + 2 - 4 * y
    barrier = pltpu.get_barrier_semaphore()

    def greet(k, _):
        pl.semaphore_signal(barrier, inc=1, device_id={"sp": lax.rem(s + k, n)}, device_id_type=MESH)
        return 0

    lax.fori_loop(1, n, greet, 0)

    def greet_other(k, _):
        pl.semaphore_signal(
            barrier, inc=1, device_id={"sp": lax.rem(s + k, n), "tp": other}, device_id_type=MESH
        )
        return 0

    lax.fori_loop(0, n, greet_other, 0)
    pltpu.make_async_copy(o_in, ow, o_sem).start()

    for j in range(n // 2):
        cols = slice(j * 2 * dim, (j + 1) * 2 * dim)
        kp, vp, qp = (r[:, cols].astype(jnp.float32) for r in (k_ref, v_ref, q_ref))
        low = lax.broadcasted_iota(jnp.int32, (rows, 2 * dim), 1) < dim
        lowh = low[:half]
        top, bot = qp[:half], qp[half:]
        sbuf[2 * j, :rows, :] = jnp.where(low, kp, pltpu.roll(vp, dim, 1)).astype(jnp.bfloat16)
        sbuf[2 * j + 1, :rows, :] = jnp.where(low, pltpu.roll(kp, dim, 1), vp).astype(jnp.bfloat16)
        sbuf[2 * j, rows:, :] = jnp.where(lowh, top, pltpu.roll(bot, dim, 1)).astype(jnp.bfloat16)
        sbuf[2 * j + 1, rows:, :] = jnp.where(lowh, pltpu.roll(top, dim, 1), bot).astype(jnp.bfloat16)

    with jax.named_scope("barrier"):
        pl.semaphore_wait(barrier, 2 * n - 1)

    def qkv_copy(t, src):
        return sends(sbuf.at[t], rbuf.at[src], qkv_s.at[t], qkv_r.at[src], {"sp": t})

    def doc_copy(t, src):
        return sends(doc_ref, docr.at[src], doc_s.at[t], doc_r.at[src], {"sp": t})

    def start_peer(k, _):
        t = lax.rem(s + k, n)
        qkv_copy(t, s).start()
        doc_copy(t, s).start()
        return 0

    lax.fori_loop(1, n, start_peer, 0)
    rbuf[pl.ds(s, 1)] = sbuf[pl.ds(s, 1)]
    docr[pl.ds(s, 1)] = doc_ref[...][None]

    mats = ((g_in, wg), (u_in, wu), (d_in, wd))
    mine = (lax.div(g, per) == c) & (y == c)

    def part_of(m, j):
        start = pl.multiple_of(j * width, width)
        return mats[m][0].at[pl.ds(start, width), :] if m == 2 else mats[m][0].at[:, pl.ds(start, width)]

    def slot_of(m, src):
        if m == 2:
            return mats[m][1].at[:, pl.ds(pl.multiple_of(src * dcols, dcols), dcols)]
        return mats[m][1].at[pl.ds(pl.multiple_of(src * depth, depth), depth), :]

    def w_copy(m, k):
        j = lax.rem(g + k, per)
        to = {"sp": 2 * (per * c + j) + x, "tp": y}
        return sends(part_of(m, j), slot_of(m, s), w_s.at[m, k], w_r.at[m, s], to)

    def own_copy(m):
        return pltpu.make_async_copy(part_of(m, lax.rem(g, per)), slot_of(m, s), own_sem.at[m])

    def start_weight(m, k):
        local = mine & (k == 0)

        @pl.when(local)
        def _():
            own_copy(m).start()

        @pl.when(jnp.logical_not(local))
        def _():
            w_copy(m, k).start()

    def start_weights(m):
        for k in range(per):
            start_weight(m, k)

    def to_x(m, src, q):
        return sends(slot_of(m, src), slot_of(m, src), wx_s.at[m, q], w_r.at[m, src], {"sp": xn})

    def to_core(m, src):
        return sends(slot_of(m, src), slot_of(m, src), wc_s.at[m, src], w_r.at[m, src], {"tp": other})

    side = lax.div(g, per)
    sided = levels // 2

    def source(q):
        there = side if q < sided else 1 - side
        return 4 * (sided * there + lax.rem(lax.div(g - c + per, 2) + levels - q, sided)) + 2 * c + x

    def hand_on(m, q):
        src = source(q)
        local = mine & (src == s)

        @pl.when(local)
        def _():
            own_copy(m).wait()

        @pl.when(jnp.logical_not(local))
        def _():
            to_core(m, src).wait_recv()

        to_x(m, src, q).start()
        to_core(m, src).start()

    def pass_on(m, q):
        src = source(q) + 1 - 2 * x
        to_core(m, src).wait_recv()
        to_core(m, src).start()

    def arrive(m):
        def arrived(k, _):
            to_core(m, 4 * lax.div(k, 2) + 2 * other + lax.rem(k, 2)).wait_recv()
            return 0

        lax.fori_loop(0, n // 2, arrived, 0)

    scale = dim ** (-0.5) * LOG2E
    off = off_ref[s] * LOG2E
    chunk = 2 * rows
    span = min(back, n - 1) + 1
    lane = lax.broadcasted_iota(jnp.int32, (half, 2 * dim), 1) < dim
    key_i = lax.broadcasted_iota(jnp.int32, (chunk, chunk), 0)
    key_j = lax.broadcasted_iota(jnp.int32, (chunk, chunk), 1)
    later = jnp.where(key_i > key_j, -1.0, 0.0).astype(jnp.bfloat16)
    query_i = lax.broadcasted_iota(jnp.int32, (rows, chunk), 0)
    before = lax.broadcasted_iota(jnp.int32, (rows, chunk), 1) - rows < query_i
    nt = (((1,), (1,)), ((), ()))

    def att_copy(t, src):
        return sends(ao.at[t], att_ref.at[src], att_s.at[t], att_r.at[src], {"sp": t})

    def scores(i):
        q2 = rbuf[i, rows:, :].astype(jnp.float32)
        q_pad = jnp.concatenate(
            [jnp.where(lane, q2, 0.0), jnp.where(lane, pltpu.roll(q2, dim, 1), 0.0)], axis=0
        ).astype(jnp.bfloat16)
        q_doc = jnp.broadcast_to(docr[i, 0:1, :].astype(jnp.float32), (rows, rows)).T
        q_doc = jnp.concatenate([q_doc, q_doc], axis=1)
        found = []
        for d in range(0, span, 2):
            js = [jnp.maximum(i - e, 0) for e in (d + 1, d)]
            kv = jnp.concatenate([rbuf[j, :rows, :] for j in js], axis=0)
            k_doc = jnp.concatenate(
                [
                    jnp.where(i >= e, docr[j, 0:1, :].astype(jnp.float32), -1.0)
                    for e, j in zip((d + 1, d), js)
                ],
                axis=1,
            )
            live = q_doc == k_doc
            if d == 0:
                live = live & before
            logit = lax.dot_general(q_pad, kv, nt, preferred_element_type=jnp.float32) * scale + off
            logit = jnp.where(live, logit, DEAD)
            drop = jnp.maximum(logit, 0.0) + jnp.log2(1.0 + jnp.exp2(-jnp.abs(logit)))
            found.append((logit - drop, drop.astype(jnp.bfloat16), jnp.sum(drop, axis=1, keepdims=True), kv))
        return found

    def weigh(i, found):
        carried = jnp.zeros((rows, 1), jnp.float32)
        weights = []
        for own, drop, dropped, _ in found:
            tail = jnp.dot(drop, later, preferred_element_type=jnp.float32)
            weights.append(jnp.exp2(own + (tail - carried)).astype(jnp.bfloat16))
            carried = carried + dropped
        total = jnp.dot(
            jnp.concatenate(weights, axis=1),
            jnp.concatenate([kv for _, _, _, kv in found], axis=0),
            preferred_element_type=jnp.float32,
        )
        packed = jnp.where(lane, pltpu.roll(total[:half], dim, 1), total[half:]).astype(jnp.bfloat16)

        @pl.when(i == s)
        def _():
            att_ref[pl.ds(s, 1)] = packed[None]

        @pl.when(i != s)
        def _():
            ao[pl.ds(i, 1)] = packed[None]
            att_copy(i, s).start()

    low = side == 0

    @pl.when(c == side)
    def _():
        for m in range(3):
            start_weights(m)


    def wait_span(src, _):
        @pl.when(src != s)
        def _():
            qkv_copy(src, src).wait_recv()
            doc_copy(src, src).wait_recv()

        return 0

    def pair(t, _):
        h = jnp.where(low, t, n // 2 - 1 - t)
        deep = jnp.maximum(2 * h + 1 - span, 0)
        deep_end = jnp.where(t == 0, n, jnp.maximum(2 * h + 3 - span, 0))
        with jax.named_scope("wait_qkv"):
            lax.fori_loop(
                jnp.where(low, 2 * h, deep), jnp.where(low, 2 * h + 2, deep_end), wait_span, 0
            )
        with jax.named_scope("att"):
            pair_steps(t)
            found = [scores(2 * h + e) for e in range(2)]
            for e in range(2):
                weigh(2 * h + e, found[e])
        return 0

    def pair_steps(t):
        @pl.when((t == 0) & (c != side))
        def _():
            for k in range(per // 2):
                start_weight(0, k)

        steps = [(m, q) for m in range(3) for q in range(sided)]
        skip = max(n // 2 - len(steps), 0)
        for i, (m, q) in enumerate(steps):
            @pl.when(t == min(skip + i, n // 2 - 1))
            def _():
                with jax.named_scope("near"):
                    hand_on(m, q)

    with jax.named_scope("attention"):
        lax.fori_loop(0, n // 2, pair, 0)

    @pl.when(c != side)
    def _():
        for k in range(per // 2, per):
            start_weight(0, k)

    def wait_attended(k, _):
        src = lax.rem(s + n - k, n)
        att_copy(src, src).wait_recv()
        return 0

    with jax.named_scope("wait_att"):
        lax.fori_loop(1, n, wait_attended, 0)
    for j in range(n // 2):
        cols = slice(j * 2 * dim, (j + 1) * 2 * dim)
        ha, hb = (att_ref[2 * j + e].astype(jnp.float32) for e in range(2))
        attd[:half, cols] = jnp.where(lane, ha, pltpu.roll(hb, dim, 1)).astype(jnp.bfloat16)
        attd[half:, cols] = jnp.where(lane, pltpu.roll(ha, dim, 1), hb).astype(jnp.bfloat16)

    pltpu.make_async_copy(o_in, ow, o_sem).wait()
    dm = ow.shape[1]
    tile = min(512, dm)

    def project(t, _):
        cols = pl.ds(pl.multiple_of(t * tile, tile), tile)
        prod = jnp.dot(attd[...], ow[:, cols], preferred_element_type=jnp.float32).astype(jnp.bfloat16)
        mixed[0, :, cols] = prod[:half]
        mixed[1, :, cols] = prod[half:]
        return 0

    with jax.named_scope("project"):
        lax.fori_loop(0, dm // tile, project, 0)
    mix = sends(mixed.at[other], mixed_in, mix_s, mix_r, {"tp": other})
    mix.start()
    with jax.named_scope("wait_mix"):
        mix.wait_recv()
    rows_f = resid_ref[...].astype(jnp.float32) + (
        mixed[c].astype(jnp.float32) + mixed_in[...].astype(jnp.float32)
    )
    stream[...] = rows_f
    inv = lax.rsqrt(jnp.mean(rows_f * rows_f, axis=1, keepdims=True) + 1e-06)
    ag[pl.ds(g, 1)] = (rows_f * inv * gain_ref[...]).astype(jnp.bfloat16)[None]

    def link(kind, k, src, dst, to):
        return sends(src, dst, net_s.at[kind, k], net_r.at[kind, k], {"sp": to})

    def up(d, zz):
        return link(0, d, ag.at[2 * zz + y], ag.at[2 * zz + y], s + 4)

    def down(d, zz):
        return link(1, d, ag.at[2 * zz + y], ag.at[2 * zz + y], s - 4)

    def across(zz):
        return link(2, zz, ag.at[2 * zz + y], ag.at[2 * zz + y], yn)

    def z_of(k):
        bit, moved = 1, z
        while bit <= k:
            if k & bit:
                moved = moved + bit - 2 * bit * lax.rem(lax.div(moved, bit), 2)
            bit *= 2
        return moved

    def rs_y(k):
        return link(3, k, part.at[2 * z_of(k) + 1 - y], fy.at[k], yn)

    def rs_z(k):
        return link(4, k, part.at[2 * z_of(k) + y], zr.at[k], s + 4 * (z_of(k) - z))

    def goes_up(d):
        return (z < levels - 1) & (z - d + 1 >= 0)

    def goes_down(d):
        return (z > 0) & (z + d - 1 < levels)

    def step_up(d):
        @pl.when(goes_up(d))
        def _():
            up(d, z - d + 1).start()

    def step_down(d):
        @pl.when(goes_down(d))
        def _():
            down(d, z + d - 1).start()

    def relay(d):
        @pl.when(z - d >= 0)
        def _():
            up(d, z - d).wait_recv()
            across(z - d).start()

        if d + 1 < levels:
            step_up(d + 1)

        @pl.when(z + d < levels)
        def _():
            down(d, z + d).wait_recv()
            across(z + d).start()

        if d + 1 < levels:
            step_down(d + 1)

    step_up(1)
    step_down(1)
    across(z).start()

    def start_far(m):
        @pl.when(c != side)
        def _():
            start_weights(m)

    def hand_far(m):
        with jax.named_scope(f"hand_far{m}"):
            for q in range(sided, levels):
                hand_on(m, q)

    start_far(1)
    hand_far(0)
    with jax.named_scope("relay1"):
        relay(1)
    start_far(2)
    hand_far(1)
    for d in range(2, levels):
        with jax.named_scope(f"relay{d}"):
            relay(d)
    for m in range(2):
        with jax.named_scope(f"pass_on{m}"):
            for q in range(levels):
                pass_on(m, q)
        with jax.named_scope(f"arrive{m}"):
            arrive(m)

    def gate_up(k):
        with jax.named_scope(f"wait_y{k}"):
            across(z_of(k)).wait_recv()
        with jax.named_scope(f"gate_up{k}"):
            xs = ag[pl.ds(2 * z_of(k), 2)].reshape(rows, dm)
            gate = jnp.dot(xs, wg[...], preferred_element_type=jnp.float32)
            upper = jnp.dot(xs, wu[...], preferred_element_type=jnp.float32)
            hid[k] = (gate / (1.0 + jnp.exp(-gate)) * upper).astype(jnp.bfloat16)

    def project_down(k):
        base = 2 * z_of(k)

        def columns(t, _):
            cols = pl.ds(pl.multiple_of(t * tile, tile), tile)
            prod = jnp.dot(hid[k], wd[:, cols], preferred_element_type=jnp.float32)
            part[pl.ds(base, 2), :, cols] = prod.astype(jnp.bfloat16).reshape(2, half, tile)
            return 0

        with jax.named_scope(f"down{k}"):
            lax.fori_loop(0, dm // tile, columns, 0)
        rs_y(k).start()

    def add(k):
        with jax.named_scope(f"add{k}"):
            rs_y(k).wait_recv()
            at = 2 * z_of(k) + y
            summed = part[at].astype(jnp.float32) + fy[k].astype(jnp.float32)
            if k == 0:
                stream[...] = stream[...] + summed
            else:
                part[at] = summed.astype(jnp.bfloat16)
                rs_z(k).start()

    for k in range(levels):
        gate_up(k)
    hand_far(2)
    with jax.named_scope("pass_on2"):
        for q in range(levels):
            pass_on(2, q)
    with jax.named_scope("arrive2"):
        arrive(2)
    order = list(range(levels - 1, -1, -1))
    for at, k in enumerate(order):
        project_down(k)
        if at > 0:
            add(order[at - 1])
    add(order[-1])
    out = stream[...]
    with jax.named_scope("wait_rs_z"):
        for k in order[:-1]:
            rs_z(k).wait_recv()
            out = out + zr[k].astype(jnp.float32)
    out_ref[...] = out.astype(jnp.bfloat16)

    with jax.named_scope("finish"):
        mix.wait_send()
        for k in range(levels):
            across(k).wait_send()
            rs_y(k).wait_send()
            if k > 0:
                rs_z(k).wait_send()

                @pl.when(goes_up(k))
                def _():
                    up(k, z - k + 1).wait_send()

                @pl.when(goes_down(k))
                def _():
                    down(k, z + k - 1).wait_send()

        def finish_peer(k, _):
            src = lax.rem(s + n - k, n)
            att_copy(src, src).wait_send()
            qkv_copy(src, src).wait_send()
            doc_copy(src, src).wait_send()
            return 0

        lax.fori_loop(1, n, finish_peer, 0)
        for m in range(3):
            for q in range(levels):
                to_x(m, source(q), q).wait_send()
                to_core(m, source(q)).wait_send()
                to_core(m, source(q) + 1 - 2 * x).wait_send()

            @pl.when(jnp.logical_not(mine))
            def _():
                w_copy(m, 0).wait_send()

            for k in range(1, per):
                w_copy(m, k).wait_send()


def resharded(
    resid, queries, keys, values, doc_ids, score_offset, out_weight, norm_gain,
    gate_weight, up_weight, down_weight,
):
    n, ntp = lax.axis_size("sp"), lax.axis_size("tp")
    rows, local = queries.shape
    half, two = rows // 2, 2 * (local // n)
    dm = resid.shape[1]
    groups, levels = n // 2, n // 4
    width = gate_weight.shape[1] * ntp // groups
    per = groups // ntp
    bf, f32 = jnp.bfloat16, jnp.float32
    vmem = pl.BlockSpec(memory_space=pltpu.VMEM)
    anyw = pl.BlockSpec(memory_space=pl.ANY)
    dma = pltpu.SemaphoreType.DMA
    block = (half, dm)
    return pl.pallas_call(
        functools.partial(layer_kernel, n),
        out_shape=jax.ShapeDtypeStruct(block, bf),
        in_specs=[vmem] * 4 + [pl.BlockSpec(memory_space=pltpu.SMEM)] + [anyw] * 3 + [vmem] * 2 + [anyw],
        out_specs=vmem,
        scratch_shapes=[
            pltpu.VMEM((n, rows + half, two), bf),
            pltpu.VMEM((n, rows + half, two), bf),
            pltpu.VMEM((n, 8, rows), jnp.int32),
            pltpu.VMEM((n, half, two), bf),
            pltpu.VMEM((n, half, two), bf),
            pltpu.VMEM((dm, width), bf),
            pltpu.VMEM((dm, width), bf),
            pltpu.VMEM((width, dm), bf),
            pltpu.VMEM(out_weight.shape, bf),
            pltpu.VMEM((rows, local), bf),
            pltpu.VMEM((2,) + block, bf),
            pltpu.VMEM(block, bf),
            pltpu.VMEM(block, f32),
            pltpu.VMEM((groups,) + block, bf),
            pltpu.VMEM((levels, rows, width), bf),
            pltpu.VMEM((groups,) + block, bf),
            pltpu.VMEM((levels,) + block, bf),
            pltpu.VMEM((levels,) + block, bf),
            dma((n,)), dma((n,)), dma((n,)), dma((n,)), dma((n,)), dma((n,)),
            dma((3, per)), dma((3, n)), dma((3, levels)), dma((3, n)), dma((3,)),
            dma, dma, dma, dma((5, levels)), dma((5, levels)),
        ],
        compiler_params=pltpu.CompilerParams(has_side_effects=True, collective_id=0, vmem_limit_bytes=60 << 20),
    )(
        queries, keys, values, jnp.broadcast_to(doc_ids[None], (8, rows)), score_offset,
        gate_weight, up_weight, down_weight, resid, norm_gain[None], out_weight,
    )


def on_device(*args):
    queries, doc_ids, score_offset, gate_weight = args[1], args[4], args[5], args[8]
    n, ntp = lax.axis_size("sp"), lax.axis_size("tp")
    dim = queries.shape[1] // score_offset.shape[0]
    fits = (
        ntp == 2
        and n >= 8
        and n & (n - 1) == 0
        and score_offset.shape[0] == n
        and 2 * dim == 128
        and doc_ids.shape[0] == 128
        and gate_weight.shape[1] * ntp % (n * 64) == 0
        and gate_weight.shape[0] % 128 == 0
    )
    return resharded(*args) if fits else windowed(*args)


def solution(mesh):
    in_specs = (
        P(("sp", "tp"), None),
        P("sp", "tp"),
        P("sp", "tp"),
        P("sp", "tp"),
        P("sp"),
        P("tp"),
        P("tp", None),
        P(),
        P("sp", "tp"),
        P("sp", "tp"),
        P("tp", "sp"),
    )
    out_specs = P(("sp", "tp"), None)
    return jax.shard_map(
        on_device, mesh=mesh, in_specs=in_specs, out_specs=out_specs, check_vma=False
    )
```

```python
import functools

import jax
import jax.numpy as jnp
from jax import lax
from jax.experimental import pallas as pl
from jax.experimental.pallas import tpu as pltpu
from jax.sharding import PartitionSpec as P


def from_behind(shard, axis, by):
    peers = lax.axis_size(axis)
    pairs = [(i, i + by) for i in range(peers) if 0 <= i + by < peers]
    return lax.ppermute(shard, axis, pairs)


def as_sent(shard):
    return jax.tree.map(lambda a: a.astype(jnp.bfloat16) if a.dtype == jnp.float32 else a, shard)


def joined(earlier, later):
    return (
        jnp.concatenate([earlier[0], later[0]], axis=0),
        jnp.concatenate([earlier[1], later[1]], axis=0),
        jnp.concatenate([earlier[2], later[2]], axis=0),
    )


def block_update(carry, block, start, context):
    queries_h, q_pos, q_docs, offsets, scale = context
    total, carried = carry
    k_block, v_block, d_block = block
    count = k_block.shape[0]
    heads = offsets.shape[0]
    head_dim = queries_h.shape[2]

    def compute():
        key_pos = start + jnp.arange(count, dtype=jnp.int32)
        live = (
            (key_pos[None, :] >= 0)
            & (key_pos[None, :] < q_pos[:, None])
            & (d_block[None, :] == q_docs[:, None])
        )
        k_heads = k_block.reshape(count, heads, head_dim)
        v_heads = v_block.reshape(count, heads, head_dim)
        scores = (
            jnp.einsum("thd,shd->hts", queries_h, k_heads, preferred_element_type=jnp.float32)
            * scale
            + offsets[:, None, None]
        )
        log_keep = jnp.where(live[None], jax.nn.log_sigmoid(-scores), 0.0)
        tail = lax.cumsum(log_keep, axis=2, reverse=True) - log_keep + carried[:, :, None]
        weight = jnp.where(live[None], jnp.exp(jax.nn.log_sigmoid(scores) + tail), 0.0).astype(
            jnp.bfloat16
        )
        added = jnp.einsum("hts,shd->thd", weight, v_heads, preferred_element_type=jnp.float32)
        return (total + added, carried + jnp.sum(log_keep, axis=2))

    reached = (start + count > 0) & (d_block[-1] >= q_docs[0])
    return lax.cond(reached, compute, lambda: carry)


def windowed(
    resid,
    queries,
    keys,
    values,
    doc_ids,
    score_offset,
    out_weight,
    norm_gain,
    gate_weight,
    up_weight,
    down_weight,
):
    rows = queries.shape[0]
    heads = score_offset.shape[0]
    head_dim = queries.shape[1] // heads
    base = lax.axis_index("sp") * rows
    q_pos = base + jnp.arange(rows, dtype=jnp.int32)
    context = (
        queries.reshape(rows, heads, head_dim),
        q_pos,
        doc_ids,
        score_offset,
        head_dim ** (-0.5),
    )
    own = (keys, values, doc_ids)
    carry = (jnp.zeros((rows, heads, head_dim), jnp.float32), jnp.zeros((heads, rows), jnp.float32))
    nearest = from_behind((keys, values, doc_ids), "sp", 1)
    paired = joined(nearest, own)
    carry = block_update(carry, paired, base - rows, context)
    middle = from_behind((paired[0], paired[1], as_sent(paired[2])), "sp", 2)
    carry = block_update(carry, middle, base - 3 * rows, context)
    fourfold = joined(middle, paired)
    farthest = from_behind((fourfold[0], fourfold[1], as_sent(fourfold[2])), "sp", 4)
    carry = block_update(
        carry, tuple((piece[2 * rows :] for piece in farthest)), base - 5 * rows, context
    )
    carry = block_update(
        carry, tuple((piece[: 2 * rows] for piece in farthest)), base - 7 * rows, context
    )
    attended = carry[0].reshape(rows, heads * head_dim).astype(jnp.bfloat16)
    mixed_attn = lax.psum_scatter(
        jnp.dot(attended, out_weight, preferred_element_type=jnp.float32).astype(jnp.bfloat16),
        "tp",
        scatter_dimension=0,
        tiled=True,
    ).astype(jnp.float32)
    stream = resid.astype(jnp.float32) + mixed_attn
    normed = (
        stream * lax.rsqrt(jnp.mean(stream * stream, axis=1, keepdims=True) + 1e-06) * norm_gain
    ).astype(jnp.bfloat16)
    span_rows = lax.all_gather(normed, "tp", axis=0, tiled=True)
    gate = jnp.dot(
        span_rows,
        lax.all_gather(gate_weight, "sp", axis=0, tiled=True),
        preferred_element_type=jnp.float32,
    )
    upper = jnp.dot(
        span_rows,
        lax.all_gather(up_weight, "sp", axis=0, tiled=True),
        preferred_element_type=jnp.float32,
    )
    hidden = (jax.nn.silu(gate) * upper).astype(jnp.bfloat16)
    partial_out = jnp.dot(
        hidden,
        lax.all_gather(down_weight, "sp", axis=1, tiled=True),
        preferred_element_type=jnp.float32,
    )
    feed = lax.psum_scatter(
        partial_out.astype(jnp.bfloat16), "tp", scatter_dimension=0, tiled=True
    ).astype(jnp.float32)
    return (stream + feed).astype(jnp.bfloat16)


DOC_MOST = 896
LOG2E = 1.4426950408889634
DEAD = -1e30
FIRST = (0, 1)
LOOP = (('S0a', 4, 0),)
AHEAD = (
    "T2", "S0b", "N00", "N01", "N10", "N11",
)
AFTER = (
    "S1a", "Y1", "S1b", "H00", "H01", "N20", "N21", "H10", "R1", "R2", "I2a", "H11", "I2b", "R3",
    "O2a", "O2b", "P00", "P01", "P02", "P03", "P10", "P11", "P12", "P13", "A00", "A01", "A02",
    "A03", "A10", "A11", "A12", "A13", "G0", "G1", "G2", "G3", "P20", "A20", "D30", "D20", "D10",
    "D00", "P21", "A21", "D31", "D21", "D11", "D01", "H20", "B30", "B31", "H21", "P22", "A22",
    "D32", "D22", "D12", "D02", "B20", "B21", "B10", "B11", "B00", "B01", "P23", "A23", "D33",
    "D23", "D13", "D03", "B32", "B12", "B02", "B33", "B22", "B23", "B13", "B03",
)
NEAREST = (0, 1, 3, 2)
MESH = pl.DeviceIdType.MESH


def sends(src, dst, send, recv, target):
    return pltpu.make_async_remote_copy(
        src_ref=src, dst_ref=dst, send_sem=send, recv_sem=recv, device_id=target, device_id_type=MESH
    )


def layer_kernel(
    n,
    q_ref, k_ref, v_ref, doc_ref, off_ref, g_in, u_in, d_in, resid_ref, gain_ref, o_in,
    out_ref,
    sbuf, rbuf, docr, ao, att_ref, wg, wu, wd, ow,
    attd, mixed, mixed_in, stream, ag, hid, part, fy, zr,
    qkv_s, qkv_r, doc_s, doc_r, att_s, att_r, w_s, w_r, wx_s, wc_s, own_sem, o_sem, mix_s, mix_r, net_s, net_r,
):
    s = lax.axis_index("sp")
    c = lax.axis_index("tp")
    rows = q_ref.shape[0]
    half = rows // 2
    dim = q_ref.shape[1] // n
    width = wg.shape[1]
    per = g_in.shape[1] // width
    depth = g_in.shape[0]
    dcols = d_in.shape[1]
    levels = n // 4
    back = -(-DOC_MOST // rows)
    other = 1 - c
    x, y, z = lax.rem(s, 2), lax.rem(lax.div(s, 2), 2), lax.div(s, 4)
    g = lax.div(s, 2)
    xn, yn = s + 1 - 2 * x, s + 2 - 4 * y
    barrier = pltpu.get_barrier_semaphore()

    def greet(k, _):
        pl.semaphore_signal(barrier, inc=1, device_id={"sp": lax.rem(s + k, n)}, device_id_type=MESH)
        return 0

    lax.fori_loop(1, n, greet, 0)

    def greet_other(k, _):
        pl.semaphore_signal(
            barrier, inc=1, device_id={"sp": lax.rem(s + k, n), "tp": other}, device_id_type=MESH
        )
        return 0

    lax.fori_loop(0, n, greet_other, 0)
    pltpu.make_async_copy(o_in, ow, o_sem).start()

    for j in range(n // 2):
        cols = slice(j * 2 * dim, (j + 1) * 2 * dim)
        kp, vp, qp = (r[:, cols].astype(jnp.float32) for r in (k_ref, v_ref, q_ref))
        low = lax.broadcasted_iota(jnp.int32, (rows, 2 * dim), 1) < dim
        lowh = low[:half]
        top, bot = qp[:half], qp[half:]
        sbuf[2 * j, :rows, :] = jnp.where(low, kp, pltpu.roll(vp, dim, 1)).astype(jnp.bfloat16)
        sbuf[2 * j + 1, :rows, :] = jnp.where(low, pltpu.roll(kp, dim, 1), vp).astype(jnp.bfloat16)
        sbuf[2 * j, rows:, :] = jnp.where(lowh, top, pltpu.roll(bot, dim, 1)).astype(jnp.bfloat16)
        sbuf[2 * j + 1, rows:, :] = jnp.where(lowh, pltpu.roll(top, dim, 1), bot).astype(jnp.bfloat16)

    with jax.named_scope("barrier"):
        pl.semaphore_wait(barrier, 2 * n - 1)

    def qkv_copy(t, src):
        return sends(sbuf.at[t], rbuf.at[src], qkv_s.at[t], qkv_r.at[src], {"sp": t})

    def doc_copy(t, src):
        return sends(doc_ref, docr.at[src], doc_s.at[t], doc_r.at[src], {"sp": t})

    def flipped(v, k):
        bit, moved = 1, v
        while bit <= k:
            if k & bit:
                moved = moved + bit - 2 * bit * lax.rem(lax.div(moved, bit), 2)
            bit *= 2
        return moved

    for kz in NEAREST:
        for kp in range(4):
            if kz + kp > 0:
                t = flipped(s, 4 * kz + kp)
                qkv_copy(t, s).start()
                doc_copy(t, s).start()
    rbuf[pl.ds(s, 1)] = sbuf[pl.ds(s, 1)]
    docr[pl.ds(s, 1)] = doc_ref[...][None]

    mats = ((g_in, wg), (u_in, wu), (d_in, wd))
    side = lax.div(g, per)
    sided = levels // 2
    mine = (side == c) & (y == c)

    def part_of(m, j):
        start = pl.multiple_of(j * width, width)
        return mats[m][0].at[pl.ds(start, width), :] if m == 2 else mats[m][0].at[:, pl.ds(start, width)]

    def slot_of(m, src):
        if m == 2:
            return mats[m][1].at[:, pl.ds(pl.multiple_of(src * dcols, dcols), dcols)]
        return mats[m][1].at[pl.ds(pl.multiple_of(src * depth, depth), depth), :]

    def w_copy(m, k):
        j = 2 * lax.rem(z + sided - lax.div(k, 2), sided) + lax.rem(y + k, 2)
        to = {"sp": 2 * (per * c + j) + x, "tp": y}
        return sends(part_of(m, j), slot_of(m, s), w_s.at[m, k], w_r.at[m, s], to)

    def own_copy(m):
        return pltpu.make_async_copy(part_of(m, lax.rem(g, per)), slot_of(m, s), own_sem.at[m])

    def start_weight(m, k):
        local = mine & (k == 0)

        @pl.when(local)
        def _():
            own_copy(m).start()

        @pl.when(jnp.logical_not(local))
        def _():
            w_copy(m, k).start()

    def start_weights(m):
        for k in range(per):
            start_weight(m, k)

    def to_x(m, src, q):
        return sends(slot_of(m, src), slot_of(m, src), wx_s.at[m, q], w_r.at[m, src], {"sp": xn})

    def to_core(m, src):
        return sends(slot_of(m, src), slot_of(m, src), wc_s.at[m, src], w_r.at[m, src], {"tp": other})


    def plane(q):
        there = side if q < sided else 1 - side
        return sided * there + lax.rem(z + q, sided)

    def source(q):
        return 4 * plane(q) + 2 * c + x

    def hand_on(m, q):
        src = source(q)
        local = mine & (src == s)

        @pl.when(local)
        def _():
            own_copy(m).wait()

        @pl.when(jnp.logical_not(local))
        def _():
            to_core(m, src).wait_recv()

        to_x(m, src, q).start()
        to_core(m, src).start()

    def pass_on(m, q):
        src = source(q) + 1 - 2 * x
        to_core(m, src).wait_recv()
        to_core(m, src).start()

    def arrive(m, q):
        for e in range(2):
            to_core(m, 4 * plane(q) + 2 * other + e).wait_recv()

    scale = dim ** (-0.5) * LOG2E
    off = off_ref[s] * LOG2E
    chunk = 2 * rows
    span = min(back, n - 1) + 1
    lane = lax.broadcasted_iota(jnp.int32, (half, 2 * dim), 1) < dim
    key_i = lax.broadcasted_iota(jnp.int32, (chunk, chunk), 0)
    key_j = lax.broadcasted_iota(jnp.int32, (chunk, chunk), 1)
    later = jnp.where(key_i > key_j, -1.0, 0.0).astype(jnp.bfloat16)
    query_i = lax.broadcasted_iota(jnp.int32, (rows, chunk), 0)
    before = lax.broadcasted_iota(jnp.int32, (rows, chunk), 1) - rows < query_i
    nt = (((1,), (1,)), ((), ()))

    def att_copy(t, src):
        return sends(ao.at[t], att_ref.at[src], att_s.at[t], att_r.at[src], {"sp": t})

    def scores(i):
        q2 = rbuf[i, rows:, :].astype(jnp.float32)
        q_pad = jnp.concatenate(
            [jnp.where(lane, q2, 0.0), jnp.where(lane, pltpu.roll(q2, dim, 1), 0.0)], axis=0
        ).astype(jnp.bfloat16)
        q_doc = jnp.broadcast_to(docr[i, 0:1, :].astype(jnp.float32), (rows, rows)).T
        q_doc = jnp.concatenate([q_doc, q_doc], axis=1)
        found = []
        for d in range(0, span, 2):
            js = [jnp.maximum(i - e, 0) for e in (d + 1, d)]
            kv = jnp.concatenate([rbuf[j, :rows, :] for j in js], axis=0)
            k_doc = jnp.concatenate(
                [
                    jnp.where(i >= e, docr[j, 0:1, :].astype(jnp.float32), -1.0)
                    for e, j in zip((d + 1, d), js)
                ],
                axis=1,
            )
            live = q_doc == k_doc
            if d == 0:
                live = live & before
            logit = lax.dot_general(q_pad, kv, nt, preferred_element_type=jnp.float32) * scale + off
            logit = jnp.where(live, logit, DEAD)
            drop = jnp.maximum(logit, 0.0) + jnp.log2(1.0 + jnp.exp2(-jnp.abs(logit)))
            found.append((logit - drop, drop.astype(jnp.bfloat16), jnp.sum(drop, axis=1, keepdims=True), kv))
        return found

    def weigh(i, found):
        carried = jnp.zeros((rows, 1), jnp.float32)
        weights = []
        for own, drop, dropped, _ in found:
            tail = jnp.dot(drop, later, preferred_element_type=jnp.float32)
            weights.append(jnp.exp2(own + (tail - carried)).astype(jnp.bfloat16))
            carried = carried + dropped
        total = jnp.dot(
            jnp.concatenate(weights, axis=1),
            jnp.concatenate([kv for _, _, _, kv in found], axis=0),
            preferred_element_type=jnp.float32,
        )
        packed = jnp.where(lane, pltpu.roll(total[:half], dim, 1), total[half:]).astype(jnp.bfloat16)

        @pl.when(i == s)
        def _():
            att_ref[pl.ds(s, 1)] = packed[None]

        @pl.when(i != s)
        def _():
            ao[pl.ds(i, 1)] = packed[None]
            att_copy(i, s).start()

    low = side == 0

    @pl.when(c == side)
    def _():
        for m in FIRST:
            start_weights(m)


    def wait_span(src, _):
        @pl.when(src != s)
        def _():
            qkv_copy(src, src).wait_recv()
            doc_copy(src, src).wait_recv()

        return 0

    def pair(t, _):
        h = jnp.where(low, t, n // 2 - 1 - t)
        deep = jnp.maximum(2 * h + 1 - span, 0)
        deep_end = jnp.where(t == 0, n, jnp.maximum(2 * h + 3 - span, 0))
        first, end = jnp.where(low, 2 * h, deep), jnp.where(low, 2 * h + 2, deep_end)
        with jax.named_scope("wait_qkv"):
            lax.fori_loop(first, end, wait_span, 0)
        with jax.named_scope("att"):
            pair_steps(t)
            found = [scores(2 * h + e) for e in range(2)]
            for e in range(2):
                weigh(2 * h + e, found[e])
        return 0

    def event(name):
        m = int(name[1])
        with jax.named_scope(name):
            if name[0] in "SIO":
                first = 0 if name[2] == "a" else per // 2
                inner = (z == sided) | (z == sided - 1)
                chosen = {"S": z >= 0, "I": inner, "O": jnp.logical_not(inner)}[name[0]]

                @pl.when((c != side) & chosen)
                def _():
                    for k in range(first, first + per // 2):
                        start_weight(m, k)
            elif name[0] == "T":
                @pl.when(c == side)
                def _():
                    start_weights(m)
            elif name[0] == "N":
                hand_on(m, int(name[2]))
            elif name[0] == "H":
                hand_on(m, sided + int(name[2]))
            elif name[0] == "P":
                pass_on(m, int(name[2]))
            elif name[0] == "A":
                arrive(m, int(name[2]))
            elif name[0] == "D":
                project_down(m, plane(int(name[2])))
            elif name[0] == "B":
                add(m, plane(int(name[2])))
            elif name[0] == "Y":
                relay(m, True)
            elif name[0] == "R":
                relay(m, False)
            elif name[0] == "G":
                gate_up(m)

    def pair_steps(t):
        for name, at_low, at_high in LOOP:
            @pl.when(t == jnp.where(low, at_low, at_high))
            def _():
                event(name)

    with jax.named_scope("attention"):
        lax.fori_loop(0, n // 2, pair, 0)

    for name in AHEAD:
        event(name)

    def wait_attended(k, _):
        src = lax.rem(s + n - k, n)
        att_copy(src, src).wait_recv()
        return 0

    with jax.named_scope("wait_att"):
        lax.fori_loop(1, n, wait_attended, 0)
    for j in range(n // 2):
        cols = slice(j * 2 * dim, (j + 1) * 2 * dim)
        ha, hb = (att_ref[2 * j + e].astype(jnp.float32) for e in range(2))
        attd[:half, cols] = jnp.where(lane, ha, pltpu.roll(hb, dim, 1)).astype(jnp.bfloat16)
        attd[half:, cols] = jnp.where(lane, pltpu.roll(ha, dim, 1), hb).astype(jnp.bfloat16)

    pltpu.make_async_copy(o_in, ow, o_sem).wait()
    dm = ow.shape[1]
    tile = min(512, dm)

    def project(t, _):
        cols = pl.ds(pl.multiple_of(t * tile, tile), tile)
        prod = jnp.dot(attd[...], ow[:, cols], preferred_element_type=jnp.float32).astype(jnp.bfloat16)
        mixed[0, :, cols] = prod[:half]
        mixed[1, :, cols] = prod[half:]
        return 0

    with jax.named_scope("project"):
        lax.fori_loop(0, dm // tile, project, 0)
    mix = sends(mixed.at[other], mixed_in, mix_s, mix_r, {"tp": other})
    mix.start()
    with jax.named_scope("wait_mix"):
        mix.wait_recv()
    rows_f = resid_ref[...].astype(jnp.float32) + (
        mixed[c].astype(jnp.float32) + mixed_in[...].astype(jnp.float32)
    )
    stream[...] = rows_f
    inv = lax.rsqrt(jnp.mean(rows_f * rows_f, axis=1, keepdims=True) + 1e-06)
    ag[pl.ds(g, 1)] = (rows_f * inv * gain_ref[...]).astype(jnp.bfloat16)[None]

    def link(kind, k, src, dst, to):
        return sends(src, dst, net_s.at[kind, k], net_r.at[kind, k], {"sp": to})

    def up(d, zz):
        return link(0, d, ag.at[2 * zz + y], ag.at[2 * zz + y], s + 4)

    def down(d, zz):
        return link(1, d, ag.at[2 * zz + y], ag.at[2 * zz + y], s - 4)

    def across(zz):
        return link(2, zz, ag.at[2 * zz + y], ag.at[2 * zz + y], yn)

    def z_of(k):
        return flipped(z, k)

    def across_part(k, h):
        at = h * levels + k
        return link(
            3, at, part.at[2 * z_of(k) + 1 - y, :, wide(h)], fy.at[k, :, wide(h)], yn
        )

    def inward(k, h):
        at = h * levels + k
        return link(
            4, at, part.at[2 * z_of(k) + y, :, wide(h)], zr.at[k, :, wide(h)], s + 4 * (z_of(k & -k) - z)
        )

    broad = dm // levels

    def wide(h):
        return pl.ds(pl.multiple_of(h * broad, broad), broad)

    def goes_up(d):
        return (z < levels - 1) & (z - d + 1 >= 0)

    def goes_down(d):
        return (z > 0) & (z + d - 1 < levels)

    def step_up(d):
        @pl.when(goes_up(d))
        def _():
            up(d, z - d + 1).start()

    def step_down(d):
        @pl.when(goes_down(d))
        def _():
            down(d, z + d - 1).start()

    def relay(d, same):
        @pl.when((z - d >= 0) & ((lax.div(z - d + levels, sided) - 2 == side) == same))
        def _():
            up(d, z - d).wait_recv()
            across(z - d).start()
            if d + 1 < levels:
                step_up(d + 1)

        @pl.when((z + d < levels) & ((lax.div(z + d, sided) == side) == same))
        def _():
            down(d, z + d).wait_recv()
            across(z + d).start()
            if d + 1 < levels:
                step_down(d + 1)

    step_up(1)
    step_down(1)
    across(z).start()

    def gate_up(k):
        with jax.named_scope(f"wait_y{k}"):
            across(z_of(k)).wait_recv()
        with jax.named_scope(f"gate_up{k}"):
            xs = ag[pl.ds(2 * z_of(k), 2)].reshape(rows, dm)
            gate = jnp.dot(xs, wg[...], preferred_element_type=jnp.float32)
            upper = jnp.dot(xs, wu[...], preferred_element_type=jnp.float32)
            hid[k] = (gate / (1.0 + jnp.exp(-gate)) * upper).astype(jnp.bfloat16)

    def project_down(k, h):
        prod = jnp.dot(hid[k], wd[:, wide(h)], preferred_element_type=jnp.float32)
        part[pl.ds(2 * z_of(k), 2), :, wide(h)] = prod.astype(jnp.bfloat16).reshape(2, half, broad)
        across_part(k, h).start()

    def add(k, h):
        across_part(k, h).wait_recv()
        at = 2 * z_of(k) + y
        summed = part[at, :, wide(h)].astype(jnp.float32) + fy[k, :, wide(h)].astype(jnp.float32)
        if k == 0:
            stream[:, wide(h)] = stream[:, wide(h)] + summed
        else:
            for j in range(k + 1, levels):
                if j - (j & -j) == k:
                    inward(j, h).wait_recv()
                    summed = summed + zr[j, :, wide(h)].astype(jnp.float32)
            part[at, :, wide(h)] = summed.astype(jnp.bfloat16)
            inward(k, h).start()

    for name in AFTER:
        event(name)
    with jax.named_scope("last"):
        for h in [plane(q) for q in range(levels)]:
            summed = stream[:, wide(h)]
            for j in range(1, levels):
                if j == j & -j:
                    inward(j, h).wait_recv()
                    summed = summed + zr[j, :, wide(h)].astype(jnp.float32)
            out_ref[:, wide(h)] = summed.astype(jnp.bfloat16)

    with jax.named_scope("finish"):
        mix.wait_send()
        for k in range(levels):
            across(k).wait_send()
            for h in range(levels):
                across_part(k, h).wait_send()
                if k > 0:
                    inward(k, h).wait_send()
            if k > 0:
                @pl.when(goes_up(k))
                def _():
                    up(k, z - k + 1).wait_send()

                @pl.when(goes_down(k))
                def _():
                    down(k, z + k - 1).wait_send()

        def finish_peer(k, _):
            src = lax.rem(s + n - k, n)
            att_copy(src, src).wait_send()
            qkv_copy(src, src).wait_send()
            doc_copy(src, src).wait_send()
            return 0

        lax.fori_loop(1, n, finish_peer, 0)
        for m in range(3):
            for q in range(levels):
                to_x(m, source(q), q).wait_send()
                to_core(m, source(q)).wait_send()
                to_core(m, source(q) + 1 - 2 * x).wait_send()

            @pl.when(jnp.logical_not(mine))
            def _():
                w_copy(m, 0).wait_send()

            for k in range(1, per):
                w_copy(m, k).wait_send()


def resharded(
    resid, queries, keys, values, doc_ids, score_offset, out_weight, norm_gain,
    gate_weight, up_weight, down_weight,
):
    n, ntp = lax.axis_size("sp"), lax.axis_size("tp")
    rows, local = queries.shape
    half, two = rows // 2, 2 * (local // n)
    dm = resid.shape[1]
    groups, levels = n // 2, n // 4
    width = gate_weight.shape[1] * ntp // groups
    per = groups // ntp
    bf, f32 = jnp.bfloat16, jnp.float32
    vmem = pl.BlockSpec(memory_space=pltpu.VMEM)
    anyw = pl.BlockSpec(memory_space=pl.ANY)
    dma = pltpu.SemaphoreType.DMA
    block = (half, dm)
    return pl.pallas_call(
        functools.partial(layer_kernel, n),
        out_shape=jax.ShapeDtypeStruct(block, bf),
        in_specs=[vmem] * 4 + [pl.BlockSpec(memory_space=pltpu.SMEM)] + [anyw] * 3 + [vmem] * 2 + [anyw],
        out_specs=vmem,
        scratch_shapes=[
            pltpu.VMEM((n, rows + half, two), bf),
            pltpu.VMEM((n, rows + half, two), bf),
            pltpu.VMEM((n, 8, rows), jnp.int32),
            pltpu.VMEM((n, half, two), bf),
            pltpu.VMEM((n, half, two), bf),
            pltpu.VMEM((dm, width), bf),
            pltpu.VMEM((dm, width), bf),
            pltpu.VMEM((width, dm), bf),
            pltpu.VMEM(out_weight.shape, bf),
            pltpu.VMEM((rows, local), bf),
            pltpu.VMEM((2,) + block, bf),
            pltpu.VMEM(block, bf),
            pltpu.VMEM(block, f32),
            pltpu.VMEM((groups,) + block, bf),
            pltpu.VMEM((levels, rows, width), bf),
            pltpu.VMEM((groups,) + block, bf),
            pltpu.VMEM((levels,) + block, bf),
            pltpu.VMEM((levels,) + block, bf),
            dma((n,)), dma((n,)), dma((n,)), dma((n,)), dma((n,)), dma((n,)),
            dma((3, per)), dma((3, n)), dma((3, levels)), dma((3, n)), dma((3,)),
            dma, dma, dma, dma((5, levels * levels)), dma((5, levels * levels)),
        ],
        compiler_params=pltpu.CompilerParams(has_side_effects=True, collective_id=0, vmem_limit_bytes=60 << 20),
    )(
        queries, keys, values, jnp.broadcast_to(doc_ids[None], (8, rows)), score_offset,
        gate_weight, up_weight, down_weight, resid, norm_gain[None], out_weight,
    )


def on_device(*args):
    queries, doc_ids, score_offset, gate_weight = args[1], args[4], args[5], args[8]
    n, ntp = lax.axis_size("sp"), lax.axis_size("tp")
    dim = queries.shape[1] // score_offset.shape[0]
    fits = (
        ntp == 2
        and n == 4 * len(NEAREST)
        and score_offset.shape[0] == n
        and 2 * dim == 128
        and doc_ids.shape[0] == 128
        and gate_weight.shape[1] * ntp % (n * 64) == 0
        and gate_weight.shape[0] % 128 == 0
    )
    return resharded(*args) if fits else windowed(*args)


def solution(mesh):
    in_specs = (
        P(("sp", "tp"), None),
        P("sp", "tp"),
        P("sp", "tp"),
        P("sp", "tp"),
        P("sp"),
        P("tp"),
        P("tp", None),
        P(),
        P("sp", "tp"),
        P("sp", "tp"),
        P("tp", "sp"),
    )
    out_specs = P(("sp", "tp"), None)
    return jax.shard_map(
        on_device, mesh=mesh, in_specs=in_specs, out_specs=out_specs, check_vma=False
    )
```

```python
import functools

import jax
import jax.numpy as jnp
from jax import lax
from jax.experimental import pallas as pl
from jax.experimental.pallas import tpu as pltpu
from jax.sharding import PartitionSpec as P


def from_behind(shard, axis, by):
    peers = lax.axis_size(axis)
    pairs = [(i, i + by) for i in range(peers) if 0 <= i + by < peers]
    return lax.ppermute(shard, axis, pairs)


def as_sent(shard):
    return jax.tree.map(lambda a: a.astype(jnp.bfloat16) if a.dtype == jnp.float32 else a, shard)


def joined(earlier, later):
    return (
        jnp.concatenate([earlier[0], later[0]], axis=0),
        jnp.concatenate([earlier[1], later[1]], axis=0),
        jnp.concatenate([earlier[2], later[2]], axis=0),
    )


def block_update(carry, block, start, context):
    queries_h, q_pos, q_docs, offsets, scale = context
    total, carried = carry
    k_block, v_block, d_block = block
    count = k_block.shape[0]
    heads = offsets.shape[0]
    head_dim = queries_h.shape[2]

    def compute():
        key_pos = start + jnp.arange(count, dtype=jnp.int32)
        live = (
            (key_pos[None, :] >= 0)
            & (key_pos[None, :] < q_pos[:, None])
            & (d_block[None, :] == q_docs[:, None])
        )
        k_heads = k_block.reshape(count, heads, head_dim)
        v_heads = v_block.reshape(count, heads, head_dim)
        scores = (
            jnp.einsum("thd,shd->hts", queries_h, k_heads, preferred_element_type=jnp.float32)
            * scale
            + offsets[:, None, None]
        )
        log_keep = jnp.where(live[None], jax.nn.log_sigmoid(-scores), 0.0)
        tail = lax.cumsum(log_keep, axis=2, reverse=True) - log_keep + carried[:, :, None]
        weight = jnp.where(live[None], jnp.exp(jax.nn.log_sigmoid(scores) + tail), 0.0).astype(
            jnp.bfloat16
        )
        added = jnp.einsum("hts,shd->thd", weight, v_heads, preferred_element_type=jnp.float32)
        return (total + added, carried + jnp.sum(log_keep, axis=2))

    reached = (start + count > 0) & (d_block[-1] >= q_docs[0])
    return lax.cond(reached, compute, lambda: carry)


def windowed(
    resid,
    queries,
    keys,
    values,
    doc_ids,
    score_offset,
    out_weight,
    norm_gain,
    gate_weight,
    up_weight,
    down_weight,
):
    rows = queries.shape[0]
    heads = score_offset.shape[0]
    head_dim = queries.shape[1] // heads
    base = lax.axis_index("sp") * rows
    q_pos = base + jnp.arange(rows, dtype=jnp.int32)
    context = (
        queries.reshape(rows, heads, head_dim),
        q_pos,
        doc_ids,
        score_offset,
        head_dim ** (-0.5),
    )
    own = (keys, values, doc_ids)
    carry = (jnp.zeros((rows, heads, head_dim), jnp.float32), jnp.zeros((heads, rows), jnp.float32))
    nearest = from_behind((keys, values, doc_ids), "sp", 1)
    paired = joined(nearest, own)
    carry = block_update(carry, paired, base - rows, context)
    middle = from_behind((paired[0], paired[1], as_sent(paired[2])), "sp", 2)
    carry = block_update(carry, middle, base - 3 * rows, context)
    fourfold = joined(middle, paired)
    farthest = from_behind((fourfold[0], fourfold[1], as_sent(fourfold[2])), "sp", 4)
    carry = block_update(
        carry, tuple((piece[2 * rows :] for piece in farthest)), base - 5 * rows, context
    )
    carry = block_update(
        carry, tuple((piece[: 2 * rows] for piece in farthest)), base - 7 * rows, context
    )
    attended = carry[0].reshape(rows, heads * head_dim).astype(jnp.bfloat16)
    mixed_attn = lax.psum_scatter(
        jnp.dot(attended, out_weight, preferred_element_type=jnp.float32).astype(jnp.bfloat16),
        "tp",
        scatter_dimension=0,
        tiled=True,
    ).astype(jnp.float32)
    stream = resid.astype(jnp.float32) + mixed_attn
    normed = (
        stream * lax.rsqrt(jnp.mean(stream * stream, axis=1, keepdims=True) + 1e-06) * norm_gain
    ).astype(jnp.bfloat16)
    span_rows = lax.all_gather(normed, "tp", axis=0, tiled=True)
    gate = jnp.dot(
        span_rows,
        lax.all_gather(gate_weight, "sp", axis=0, tiled=True),
        preferred_element_type=jnp.float32,
    )
    upper = jnp.dot(
        span_rows,
        lax.all_gather(up_weight, "sp", axis=0, tiled=True),
        preferred_element_type=jnp.float32,
    )
    hidden = (jax.nn.silu(gate) * upper).astype(jnp.bfloat16)
    partial_out = jnp.dot(
        hidden,
        lax.all_gather(down_weight, "sp", axis=1, tiled=True),
        preferred_element_type=jnp.float32,
    )
    feed = lax.psum_scatter(
        partial_out.astype(jnp.bfloat16), "tp", scatter_dimension=0, tiled=True
    ).astype(jnp.float32)
    return (stream + feed).astype(jnp.bfloat16)


DOC_MOST = 896
LOG2E = 1.4426950408889634
DEAD = -1e30
FIRST = (0, 1)
LOOP = (('S0a', 4, 0),)
AHEAD = (
    "T2", "S0b", "N00", "N01", "N10", "N11",
)
AFTER = (
    "S1a", "Y1", "S1b", "H00", "H01", "N20", "N21", "H10", "R1", "R2", "I2a", "P00", "P01", "P10",
    "P11", "P20", "P21", "H11", "I2b", "R3", "O2a", "O2b", "P02", "P03", "P12", "P13", "A20", "A21",
    "A00", "A01", "A02", "A03", "A10", "A11", "A12", "A13", "G2", "D20", "D21", "G3", "D30", "D31",
    "H20", "G1", "D10", "D11", "H21", "G0", "D00", "D01", "B30", "B31", "P22", "A22", "D32", "D22",
    "B20", "B21", "B10", "B11", "P23", "A23", "D33", "D23", "D12", "D13", "D02", "D03", "B00",
    "B01", "B32", "B22", "B33", "B23", "B12", "B13", "B02", "B03",
)
NEAREST = (0, 1, 3, 2)
MESH = pl.DeviceIdType.MESH


def sends(src, dst, send, recv, target):
    return pltpu.make_async_remote_copy(
        src_ref=src, dst_ref=dst, send_sem=send, recv_sem=recv, device_id=target, device_id_type=MESH
    )


def layer_kernel(
    n,
    q_ref, k_ref, v_ref, doc_ref, off_ref, g_in, u_in, d_in, resid_ref, gain_ref, o_in,
    out_ref,
    sbuf, rbuf, docr, ao, att_ref, wg, wu, wd, ow,
    attd, mixed, mixed_in, stream, ag, hid, part, fy, zr,
    qkv_s, qkv_r, doc_s, doc_r, att_s, att_r, w_s, w_r, wx_s, wc_s, own_sem, o_sem, mix_s, mix_r, net_s, net_r,
):
    s = lax.axis_index("sp")
    c = lax.axis_index("tp")
    rows = q_ref.shape[0]
    half = rows // 2
    dim = q_ref.shape[1] // n
    width = wg.shape[1]
    per = g_in.shape[1] // width
    depth = g_in.shape[0]
    dcols = d_in.shape[1]
    levels = n // 4
    back = -(-DOC_MOST // rows)
    other = 1 - c
    x, y, z = lax.rem(s, 2), lax.rem(lax.div(s, 2), 2), lax.div(s, 4)
    g = lax.div(s, 2)
    xn, yn = s + 1 - 2 * x, s + 2 - 4 * y
    barrier = pltpu.get_barrier_semaphore()

    def greet(k, _):
        pl.semaphore_signal(barrier, inc=1, device_id={"sp": lax.rem(s + k, n)}, device_id_type=MESH)
        return 0

    lax.fori_loop(1, n, greet, 0)

    def greet_other(k, _):
        pl.semaphore_signal(
            barrier, inc=1, device_id={"sp": lax.rem(s + k, n), "tp": other}, device_id_type=MESH
        )
        return 0

    lax.fori_loop(0, n, greet_other, 0)
    pltpu.make_async_copy(o_in, ow, o_sem).start()

    for j in range(n // 2):
        cols = slice(j * 2 * dim, (j + 1) * 2 * dim)
        kp, vp, qp = (r[:, cols].astype(jnp.float32) for r in (k_ref, v_ref, q_ref))
        low = lax.broadcasted_iota(jnp.int32, (rows, 2 * dim), 1) < dim
        lowh = low[:half]
        top, bot = qp[:half], qp[half:]
        sbuf[2 * j, :rows, :] = jnp.where(low, kp, pltpu.roll(vp, dim, 1)).astype(jnp.bfloat16)
        sbuf[2 * j + 1, :rows, :] = jnp.where(low, pltpu.roll(kp, dim, 1), vp).astype(jnp.bfloat16)
        sbuf[2 * j, rows:, :] = jnp.where(lowh, top, pltpu.roll(bot, dim, 1)).astype(jnp.bfloat16)
        sbuf[2 * j + 1, rows:, :] = jnp.where(lowh, pltpu.roll(top, dim, 1), bot).astype(jnp.bfloat16)

    with jax.named_scope("barrier"):
        pl.semaphore_wait(barrier, 2 * n - 1)

    def qkv_copy(t, src):
        return sends(sbuf.at[t], rbuf.at[src], qkv_s.at[t], qkv_r.at[src], {"sp": t})

    def doc_copy(t, src):
        return sends(doc_ref, docr.at[src], doc_s.at[t], doc_r.at[src], {"sp": t})

    def flipped(v, k):
        bit, moved = 1, v
        while bit <= k:
            if k & bit:
                moved = moved + bit - 2 * bit * lax.rem(lax.div(moved, bit), 2)
            bit *= 2
        return moved

    for kz in NEAREST:
        for kp in range(4):
            if kz + kp > 0:
                t = flipped(s, 4 * kz + kp)
                qkv_copy(t, s).start()
                doc_copy(t, s).start()
    rbuf[pl.ds(s, 1)] = sbuf[pl.ds(s, 1)]
    docr[pl.ds(s, 1)] = doc_ref[...][None]

    mats = ((g_in, wg), (u_in, wu), (d_in, wd), (d_in, wd))
    deep = width // 2
    side = lax.div(g, per)
    sided = levels // 2
    mine = (side == c) & (y == c)

    def part_of(m, j):
        if m >= 2:
            return d_in.at[pl.ds(pl.multiple_of(j * width + (m - 2) * deep, deep), deep), :]
        return mats[m][0].at[:, pl.ds(pl.multiple_of(j * width, width), width)]

    def slot_of(m, src):
        if m >= 2:
            return wd.at[pl.ds((m - 2) * deep, deep), pl.ds(pl.multiple_of(src * dcols, dcols), dcols)]
        return mats[m][1].at[pl.ds(pl.multiple_of(src * depth, depth), depth), :]

    def w_copy(m, k):
        j = 2 * lax.rem(z + sided - lax.div(k, 2), sided) + lax.rem(y + k, 2)
        to = {"sp": 2 * (per * c + j) + x, "tp": y}
        return sends(part_of(m, j), slot_of(m, s), w_s.at[m, k], w_r.at[m, s], to)

    def own_copy(m):
        return pltpu.make_async_copy(part_of(m, lax.rem(g, per)), slot_of(m, s), own_sem.at[m])

    def parts(m):
        return (2, 3) if m == 2 else (m,)

    def start_weight(m, k):
        for e in parts(m):
            start_part(e, k)

    def start_part(m, k):
        local = mine & (k == 0)

        @pl.when(local)
        def _():
            own_copy(m).start()

        @pl.when(jnp.logical_not(local))
        def _():
            w_copy(m, k).start()

    def start_weights(m):
        for k in range(per):
            start_weight(m, k)

    def to_x(m, src, q):
        return sends(slot_of(m, src), slot_of(m, src), wx_s.at[m, q], w_r.at[m, src], {"sp": xn})

    def to_core(m, src):
        return sends(slot_of(m, src), slot_of(m, src), wc_s.at[m, src], w_r.at[m, src], {"tp": other})


    def plane(q):
        there = side if q < sided else 1 - side
        return sided * there + lax.rem(z + q, sided)

    def source(q):
        return 4 * plane(q) + 2 * c + x

    def hand_on(m, q):
        for e in parts(m):
            hand_part(e, q)

    def hand_part(m, q):
        src = source(q)
        local = mine & (src == s)

        @pl.when(local)
        def _():
            own_copy(m).wait()

        @pl.when(jnp.logical_not(local))
        def _():
            to_core(m, src).wait_recv()

        to_x(m, src, q).start()
        to_core(m, src).start()

    def pass_on(m, q):
        src = source(q) + 1 - 2 * x
        for e in parts(m):
            to_core(e, src).wait_recv()
            to_core(e, src).start()

    def arrive(m, q):
        for p in parts(m):
            for e in range(2):
                to_core(p, 4 * plane(q) + 2 * other + e).wait_recv()

    scale = dim ** (-0.5) * LOG2E
    off = off_ref[s] * LOG2E
    chunk = 2 * rows
    span = min(back, n - 1) + 1
    lane = lax.broadcasted_iota(jnp.int32, (half, 2 * dim), 1) < dim
    key_i = lax.broadcasted_iota(jnp.int32, (chunk, chunk), 0)
    key_j = lax.broadcasted_iota(jnp.int32, (chunk, chunk), 1)
    later = jnp.where(key_i > key_j, -1.0, 0.0).astype(jnp.bfloat16)
    query_i = lax.broadcasted_iota(jnp.int32, (rows, chunk), 0)
    before = lax.broadcasted_iota(jnp.int32, (rows, chunk), 1) - rows < query_i
    nt = (((1,), (1,)), ((), ()))

    def att_copy(t, src):
        return sends(ao.at[t], att_ref.at[src], att_s.at[t], att_r.at[src], {"sp": t})

    def scores(i):
        q2 = rbuf[i, rows:, :].astype(jnp.float32)
        q_pad = jnp.concatenate(
            [jnp.where(lane, q2, 0.0), jnp.where(lane, pltpu.roll(q2, dim, 1), 0.0)], axis=0
        ).astype(jnp.bfloat16)
        q_doc = jnp.broadcast_to(docr[i, 0:1, :].astype(jnp.float32), (rows, rows)).T
        q_doc = jnp.concatenate([q_doc, q_doc], axis=1)
        found = []
        for d in range(0, span, 2):
            js = [jnp.maximum(i - e, 0) for e in (d + 1, d)]
            kv = jnp.concatenate([rbuf[j, :rows, :] for j in js], axis=0)
            k_doc = jnp.concatenate(
                [
                    jnp.where(i >= e, docr[j, 0:1, :].astype(jnp.float32), -1.0)
                    for e, j in zip((d + 1, d), js)
                ],
                axis=1,
            )
            live = q_doc == k_doc
            if d == 0:
                live = live & before
            logit = lax.dot_general(q_pad, kv, nt, preferred_element_type=jnp.float32) * scale + off
            logit = jnp.where(live, logit, DEAD)
            drop = jnp.maximum(logit, 0.0) + jnp.log2(1.0 + jnp.exp2(-jnp.abs(logit)))
            found.append((logit - drop, drop.astype(jnp.bfloat16), jnp.sum(drop, axis=1, keepdims=True), kv))
        return found

    def weigh(i, found):
        carried = jnp.zeros((rows, 1), jnp.float32)
        weights = []
        for own, drop, dropped, _ in found:
            tail = jnp.dot(drop, later, preferred_element_type=jnp.float32)
            weights.append(jnp.exp2(own + (tail - carried)).astype(jnp.bfloat16))
            carried = carried + dropped
        total = jnp.dot(
            jnp.concatenate(weights, axis=1),
            jnp.concatenate([kv for _, _, _, kv in found], axis=0),
            preferred_element_type=jnp.float32,
        )
        packed = jnp.where(lane, pltpu.roll(total[:half], dim, 1), total[half:]).astype(jnp.bfloat16)

        @pl.when(i == s)
        def _():
            att_ref[pl.ds(s, 1)] = packed[None]

        @pl.when(i != s)
        def _():
            ao[pl.ds(i, 1)] = packed[None]
            att_copy(i, s).start()

    low = side == 0

    @pl.when(c == side)
    def _():
        for m in FIRST:
            start_weights(m)


    def wait_span(src, _):
        @pl.when(src != s)
        def _():
            qkv_copy(src, src).wait_recv()
            doc_copy(src, src).wait_recv()

        return 0

    def pair(t, _):
        h = jnp.where(low, t, n // 2 - 1 - t)
        deep = jnp.maximum(2 * h + 1 - span, 0)
        deep_end = jnp.where(t == 0, n, jnp.maximum(2 * h + 3 - span, 0))
        first, end = jnp.where(low, 2 * h, deep), jnp.where(low, 2 * h + 2, deep_end)
        with jax.named_scope("wait_qkv"):
            lax.fori_loop(first, end, wait_span, 0)
        with jax.named_scope("att"):
            pair_steps(t)
            found = [scores(2 * h + e) for e in range(2)]
            for e in range(2):
                weigh(2 * h + e, found[e])
        return 0

    def event(name):
        m = int(name[1])
        with jax.named_scope(name):
            if name[0] in "SIO":
                first = 0 if name[2] == "a" else per // 2
                inner = (z == sided) | (z == sided - 1)
                chosen = {"S": z >= 0, "I": inner, "O": jnp.logical_not(inner)}[name[0]]

                @pl.when((c != side) & chosen)
                def _():
                    for k in range(first, first + per // 2):
                        start_weight(m, k)
            elif name[0] == "T":
                @pl.when(c == side)
                def _():
                    start_weights(m)
            elif name[0] == "N":
                hand_on(m, int(name[2]))
            elif name[0] == "H":
                hand_on(m, sided + int(name[2]))
            elif name[0] == "P":
                pass_on(m, int(name[2]))
            elif name[0] == "A":
                arrive(m, int(name[2]))
            elif name[0] == "D":
                project_down(m, plane(int(name[2])))
            elif name[0] == "B":
                add(m, int(name[2]))
            elif name[0] == "Y":
                relay(m, True)
            elif name[0] == "R":
                relay(m, False)
            elif name[0] == "G":
                gate_up(m)

    def pair_steps(t):
        for name, at_low, at_high in LOOP:
            @pl.when(t == jnp.where(low, at_low, at_high))
            def _():
                event(name)

    with jax.named_scope("attention"):
        lax.fori_loop(0, n // 2, pair, 0)

    for name in AHEAD:
        event(name)

    def wait_attended(k, _):
        src = lax.rem(s + n - k, n)
        att_copy(src, src).wait_recv()
        return 0

    with jax.named_scope("wait_att"):
        lax.fori_loop(1, n, wait_attended, 0)
    for j in range(n // 2):
        cols = slice(j * 2 * dim, (j + 1) * 2 * dim)
        ha, hb = (att_ref[2 * j + e].astype(jnp.float32) for e in range(2))
        attd[:half, cols] = jnp.where(lane, ha, pltpu.roll(hb, dim, 1)).astype(jnp.bfloat16)
        attd[half:, cols] = jnp.where(lane, pltpu.roll(ha, dim, 1), hb).astype(jnp.bfloat16)

    pltpu.make_async_copy(o_in, ow, o_sem).wait()
    dm = ow.shape[1]
    tile = min(512, dm)

    def project(t, _):
        cols = pl.ds(pl.multiple_of(t * tile, tile), tile)
        prod = jnp.dot(attd[...], ow[:, cols], preferred_element_type=jnp.float32).astype(jnp.bfloat16)
        mixed[0, :, cols] = prod[:half]
        mixed[1, :, cols] = prod[half:]
        return 0

    with jax.named_scope("project"):
        lax.fori_loop(0, dm // tile, project, 0)
    mix = sends(mixed.at[other], mixed_in, mix_s, mix_r, {"tp": other})
    mix.start()
    with jax.named_scope("wait_mix"):
        mix.wait_recv()
    rows_f = resid_ref[...].astype(jnp.float32) + (
        mixed[c].astype(jnp.float32) + mixed_in[...].astype(jnp.float32)
    )
    stream[...] = rows_f
    inv = lax.rsqrt(jnp.mean(rows_f * rows_f, axis=1, keepdims=True) + 1e-06)
    ag[pl.ds(g, 1)] = (rows_f * inv * gain_ref[...]).astype(jnp.bfloat16)[None]

    def link(kind, k, src, dst, to):
        return sends(src, dst, net_s.at[kind, k], net_r.at[kind, k], {"sp": to})

    def up(d, zz):
        return link(0, d, ag.at[2 * zz + y], ag.at[2 * zz + y], s + 4)

    def down(d, zz):
        return link(1, d, ag.at[2 * zz + y], ag.at[2 * zz + y], s - 4)

    def across(zz):
        return link(2, zz, ag.at[2 * zz + y], ag.at[2 * zz + y], yn)

    def z_of(k):
        return flipped(z, k)

    def across_part(k, h):
        at = h * levels + k
        return link(
            3, at, part.at[2 * z_of(k) + 1 - y, :, wide(h)], fy.at[k, :, wide(h)], yn
        )

    def inward(k, h):
        at = h * levels + k
        return link(
            4, at, part.at[2 * z_of(k) + y, :, wide(h)], zr.at[k, :, wide(h)], s + 4 * (z_of(k & -k) - z)
        )

    broad = dm // levels

    def wide(h):
        return pl.ds(pl.multiple_of(h * broad, broad), broad)

    def goes_up(d):
        return (z < levels - 1) & (z - d + 1 >= 0)

    def goes_down(d):
        return (z > 0) & (z + d - 1 < levels)

    def step_up(d):
        @pl.when(goes_up(d))
        def _():
            up(d, z - d + 1).start()

    def step_down(d):
        @pl.when(goes_down(d))
        def _():
            down(d, z + d - 1).start()

    def relay(d, same):
        @pl.when((z - d >= 0) & ((lax.div(z - d + levels, sided) - 2 == side) == same))
        def _():
            up(d, z - d).wait_recv()
            across(z - d).start()
            if d + 1 < levels:
                step_up(d + 1)

        @pl.when((z + d < levels) & ((lax.div(z + d, sided) == side) == same))
        def _():
            down(d, z + d).wait_recv()
            across(z + d).start()
            if d + 1 < levels:
                step_down(d + 1)

    step_up(1)
    step_down(1)
    across(z).start()

    def gate_up(k):
        with jax.named_scope(f"wait_y{k}"):
            across(z_of(k)).wait_recv()
        with jax.named_scope(f"gate_up{k}"):
            xs = ag[pl.ds(2 * z_of(k), 2)].reshape(rows, dm)
            gate = jnp.dot(xs, wg[...], preferred_element_type=jnp.float32)
            upper = jnp.dot(xs, wu[...], preferred_element_type=jnp.float32)
            hid[k] = (gate / (1.0 + jnp.exp(-gate)) * upper).astype(jnp.bfloat16)

    def project_down(k, h):
        prod = jnp.dot(hid[k], wd[:, wide(h)], preferred_element_type=jnp.float32)
        part[pl.ds(2 * z_of(k), 2), :, wide(h)] = prod.astype(jnp.bfloat16).reshape(2, half, broad)
        across_part(k, h).start()

    def direct(h):
        far = z_of(levels - 1)
        return link(4, h * levels, part.at[2 * far + y, :, wide(h)], zr.at[0, :, wide(h)], s + 4 * (far - z))

    def outward(k, q):
        h = plane(q)
        return direct(h) if k == q == levels - 1 else inward(k, h)

    def add(k, q):
        h = plane(q)
        across_part(k, h).wait_recv()
        at = 2 * z_of(k) + y
        summed = part[at, :, wide(h)].astype(jnp.float32) + fy[k, :, wide(h)].astype(jnp.float32)
        if k == 0:
            stream[:, wide(h)] = stream[:, wide(h)] + summed
        else:
            if k == levels - 2 and q != levels - 2:
                inward(k + 1, h).wait_recv()
                summed = summed + zr[k + 1, :, wide(h)].astype(jnp.float32)
            part[at, :, wide(h)] = summed.astype(jnp.bfloat16)
            outward(k, q).start()

    for name in AFTER:
        event(name)
    with jax.named_scope("last"):
        for q in range(levels):
            h = plane(q)
            summed = stream[:, wide(h)]
            for j in range(1, levels):
                if j == j & -j:
                    inward(j, h).wait_recv()
                    summed = summed + zr[j, :, wide(h)].astype(jnp.float32)
            if q == 0:
                direct(h).wait_recv()
                summed = summed + zr[0, :, wide(h)].astype(jnp.float32)
            out_ref[:, wide(h)] = summed.astype(jnp.bfloat16)

    with jax.named_scope("finish"):
        mix.wait_send()
        for k in range(levels):
            across(k).wait_send()
            for q in range(levels):
                across_part(k, plane(q)).wait_send()
                if k > 0:
                    outward(k, q).wait_send()
            if k > 0:
                @pl.when(goes_up(k))
                def _():
                    up(k, z - k + 1).wait_send()

                @pl.when(goes_down(k))
                def _():
                    down(k, z + k - 1).wait_send()

        def finish_peer(k, _):
            src = lax.rem(s + n - k, n)
            att_copy(src, src).wait_send()
            qkv_copy(src, src).wait_send()
            doc_copy(src, src).wait_send()
            return 0

        lax.fori_loop(1, n, finish_peer, 0)
        for m in range(len(mats)):
            for q in range(levels):
                to_x(m, source(q), q).wait_send()
                to_core(m, source(q)).wait_send()
                to_core(m, source(q) + 1 - 2 * x).wait_send()

            @pl.when(jnp.logical_not(mine))
            def _():
                w_copy(m, 0).wait_send()

            for k in range(1, per):
                w_copy(m, k).wait_send()


def resharded(
    resid, queries, keys, values, doc_ids, score_offset, out_weight, norm_gain,
    gate_weight, up_weight, down_weight,
):
    n, ntp = lax.axis_size("sp"), lax.axis_size("tp")
    rows, local = queries.shape
    half, two = rows // 2, 2 * (local // n)
    dm = resid.shape[1]
    groups, levels = n // 2, n // 4
    width = gate_weight.shape[1] * ntp // groups
    per = groups // ntp
    bf, f32 = jnp.bfloat16, jnp.float32
    vmem = pl.BlockSpec(memory_space=pltpu.VMEM)
    anyw = pl.BlockSpec(memory_space=pl.ANY)
    dma = pltpu.SemaphoreType.DMA
    block = (half, dm)
    return pl.pallas_call(
        functools.partial(layer_kernel, n),
        out_shape=jax.ShapeDtypeStruct(block, bf),
        in_specs=[vmem] * 4 + [pl.BlockSpec(memory_space=pltpu.SMEM)] + [anyw] * 3 + [vmem] * 2 + [anyw],
        out_specs=vmem,
        scratch_shapes=[
            pltpu.VMEM((n, rows + half, two), bf),
            pltpu.VMEM((n, rows + half, two), bf),
            pltpu.VMEM((n, 1, rows), jnp.int32),
            pltpu.VMEM((n, half, two), bf),
            pltpu.VMEM((n, half, two), bf),
            pltpu.VMEM((dm, width), bf),
            pltpu.VMEM((dm, width), bf),
            pltpu.VMEM((width, dm), bf),
            pltpu.VMEM(out_weight.shape, bf),
            pltpu.VMEM((rows, local), bf),
            pltpu.VMEM((2,) + block, bf),
            pltpu.VMEM(block, bf),
            pltpu.VMEM(block, f32),
            pltpu.VMEM((groups,) + block, bf),
            pltpu.VMEM((levels, rows, width), bf),
            pltpu.VMEM((groups,) + block, bf),
            pltpu.VMEM((levels,) + block, bf),
            pltpu.VMEM((levels,) + block, bf),
            dma((n,)), dma((n,)), dma((n,)), dma((n,)), dma((n,)), dma((n,)),
            dma((4, per)), dma((4, n)), dma((4, levels)), dma((4, n)), dma((4,)),
            dma, dma, dma, dma((5, levels * levels)), dma((5, levels * levels)),
        ],
        compiler_params=pltpu.CompilerParams(has_side_effects=True, collective_id=0, vmem_limit_bytes=60 << 20),
    )(
        queries, keys, values, doc_ids[None], score_offset,
        gate_weight, up_weight, down_weight, resid, norm_gain[None], out_weight,
    )


def on_device(*args):
    queries, doc_ids, score_offset, gate_weight = args[1], args[4], args[5], args[8]
    n, ntp = lax.axis_size("sp"), lax.axis_size("tp")
    dim = queries.shape[1] // score_offset.shape[0]
    fits = (
        ntp == 2
        and n == 4 * len(NEAREST)
        and score_offset.shape[0] == n
        and 2 * dim == 128
        and doc_ids.shape[0] == 128
        and gate_weight.shape[1] * ntp % (n * 64) == 0
        and gate_weight.shape[0] % 128 == 0
    )
    return resharded(*args) if fits else windowed(*args)


def solution(mesh):
    in_specs = (
        P(("sp", "tp"), None),
        P("sp", "tp"),
        P("sp", "tp"),
        P("sp", "tp"),
        P("sp"),
        P("tp"),
        P("tp", None),
        P(),
        P("sp", "tp"),
        P("sp", "tp"),
        P("tp", "sp"),
    )
    out_specs = P(("sp", "tp"), None)
    return jax.shard_map(
        on_device, mesh=mesh, in_specs=in_specs, out_specs=out_specs, check_vma=False
    )
```

```python
import functools

import jax
import jax.numpy as jnp
from jax import lax
from jax.experimental import pallas as pl
from jax.experimental.pallas import tpu as pltpu
from jax.sharding import PartitionSpec as P


def from_behind(shard, axis, by):
    peers = lax.axis_size(axis)
    pairs = [(i, i + by) for i in range(peers) if 0 <= i + by < peers]
    return lax.ppermute(shard, axis, pairs)


def as_sent(shard):
    return jax.tree.map(lambda a: a.astype(jnp.bfloat16) if a.dtype == jnp.float32 else a, shard)


def joined(earlier, later):
    return (
        jnp.concatenate([earlier[0], later[0]], axis=0),
        jnp.concatenate([earlier[1], later[1]], axis=0),
        jnp.concatenate([earlier[2], later[2]], axis=0),
    )


def block_update(carry, block, start, context):
    queries_h, q_pos, q_docs, offsets, scale = context
    total, carried = carry
    k_block, v_block, d_block = block
    count = k_block.shape[0]
    heads = offsets.shape[0]
    head_dim = queries_h.shape[2]

    def compute():
        key_pos = start + jnp.arange(count, dtype=jnp.int32)
        live = (
            (key_pos[None, :] >= 0)
            & (key_pos[None, :] < q_pos[:, None])
            & (d_block[None, :] == q_docs[:, None])
        )
        k_heads = k_block.reshape(count, heads, head_dim)
        v_heads = v_block.reshape(count, heads, head_dim)
        scores = (
            jnp.einsum("thd,shd->hts", queries_h, k_heads, preferred_element_type=jnp.float32)
            * scale
            + offsets[:, None, None]
        )
        log_keep = jnp.where(live[None], jax.nn.log_sigmoid(-scores), 0.0)
        tail = lax.cumsum(log_keep, axis=2, reverse=True) - log_keep + carried[:, :, None]
        weight = jnp.where(live[None], jnp.exp(jax.nn.log_sigmoid(scores) + tail), 0.0).astype(
            jnp.bfloat16
        )
        added = jnp.einsum("hts,shd->thd", weight, v_heads, preferred_element_type=jnp.float32)
        return (total + added, carried + jnp.sum(log_keep, axis=2))

    reached = (start + count > 0) & (d_block[-1] >= q_docs[0])
    return lax.cond(reached, compute, lambda: carry)


def windowed(
    resid,
    queries,
    keys,
    values,
    doc_ids,
    score_offset,
    out_weight,
    norm_gain,
    gate_weight,
    up_weight,
    down_weight,
):
    rows = queries.shape[0]
    heads = score_offset.shape[0]
    head_dim = queries.shape[1] // heads
    base = lax.axis_index("sp") * rows
    q_pos = base + jnp.arange(rows, dtype=jnp.int32)
    context = (
        queries.reshape(rows, heads, head_dim),
        q_pos,
        doc_ids,
        score_offset,
        head_dim ** (-0.5),
    )
    own = (keys, values, doc_ids)
    carry = (jnp.zeros((rows, heads, head_dim), jnp.float32), jnp.zeros((heads, rows), jnp.float32))
    nearest = from_behind((keys, values, doc_ids), "sp", 1)
    paired = joined(nearest, own)
    carry = block_update(carry, paired, base - rows, context)
    middle = from_behind((paired[0], paired[1], as_sent(paired[2])), "sp", 2)
    carry = block_update(carry, middle, base - 3 * rows, context)
    fourfold = joined(middle, paired)
    farthest = from_behind((fourfold[0], fourfold[1], as_sent(fourfold[2])), "sp", 4)
    carry = block_update(
        carry, tuple((piece[2 * rows :] for piece in farthest)), base - 5 * rows, context
    )
    carry = block_update(
        carry, tuple((piece[: 2 * rows] for piece in farthest)), base - 7 * rows, context
    )
    attended = carry[0].reshape(rows, heads * head_dim).astype(jnp.bfloat16)
    mixed_attn = lax.psum_scatter(
        jnp.dot(attended, out_weight, preferred_element_type=jnp.float32).astype(jnp.bfloat16),
        "tp",
        scatter_dimension=0,
        tiled=True,
    ).astype(jnp.float32)
    stream = resid.astype(jnp.float32) + mixed_attn
    normed = (
        stream * lax.rsqrt(jnp.mean(stream * stream, axis=1, keepdims=True) + 1e-06) * norm_gain
    ).astype(jnp.bfloat16)
    span_rows = lax.all_gather(normed, "tp", axis=0, tiled=True)
    gate = jnp.dot(
        span_rows,
        lax.all_gather(gate_weight, "sp", axis=0, tiled=True),
        preferred_element_type=jnp.float32,
    )
    upper = jnp.dot(
        span_rows,
        lax.all_gather(up_weight, "sp", axis=0, tiled=True),
        preferred_element_type=jnp.float32,
    )
    hidden = (jax.nn.silu(gate) * upper).astype(jnp.bfloat16)
    partial_out = jnp.dot(
        hidden,
        lax.all_gather(down_weight, "sp", axis=1, tiled=True),
        preferred_element_type=jnp.float32,
    )
    feed = lax.psum_scatter(
        partial_out.astype(jnp.bfloat16), "tp", scatter_dimension=0, tiled=True
    ).astype(jnp.float32)
    return (stream + feed).astype(jnp.bfloat16)


DOC_MOST = 896
LOG2E = 1.4426950408889634
DEAD = -1e30
FIRST = (0, 1)
LOOP = (('S0a', 5, 1),)
AHEAD = (
    "T2", "S0b", "N00", "N01", "N10", "N11",
)
AFTER = (
    "S1a", "Y1", "S1b", "H00", "H01", "N20", "N21", "H10", "R1", "R2", "I2a", "P00", "P01", "P10",
    "P11", "P20", "P21", "H11", "I2b", "R3", "O2a", "O2b", "P02", "P03", "P12", "P13", "A20", "A21",
    "A00", "A01", "A02", "A03", "A10", "A11", "A12", "A13", "G2", "D20", "D21", "G3", "D30", "D31",
    "H20", "G1", "D10", "D11", "H21", "G0", "D00", "D01", "B30", "B31", "P22", "A22", "D32", "D22",
    "B20", "B21", "B10", "B11", "P23", "A23", "D33", "D23", "D12", "D13", "D02", "D03", "B00",
    "B01", "B32", "B22", "B33", "B23", "B12", "B13", "B02", "B03",
)
NEAREST = (0, 1, 3, 2)
MESH = pl.DeviceIdType.MESH


def sends(src, dst, send, recv, target):
    return pltpu.make_async_remote_copy(
        src_ref=src, dst_ref=dst, send_sem=send, recv_sem=recv, device_id=target, device_id_type=MESH
    )


def layer_kernel(
    n,
    q_ref, k_ref, v_ref, doc_ref, off_ref, g_in, u_in, d_in, resid_ref, gain_ref, o_in,
    out_ref,
    sbuf, rbuf, docr, ao, att_ref, wg, wu, wd, ow,
    attd, mixed, mixed_in, stream, ag, hid, part, fy, zr,
    qkv_s, qkv_r, doc_s, doc_r, att_s, att_r, w_s, w_r, wx_s, wc_s, own_sem, o_sem, mix_s, mix_r, net_s, net_r,
):
    s = lax.axis_index("sp")
    c = lax.axis_index("tp")
    rows = q_ref.shape[0]
    half = rows // 2
    dim = q_ref.shape[1] // n
    width = wg.shape[1]
    per = g_in.shape[1] // width
    depth = g_in.shape[0]
    dcols = d_in.shape[1]
    levels = n // 4
    back = -(-DOC_MOST // rows)
    other = 1 - c
    x, y, z = lax.rem(s, 2), lax.rem(lax.div(s, 2), 2), lax.div(s, 4)
    g = lax.div(s, 2)
    xn, yn = s + 1 - 2 * x, s + 2 - 4 * y
    barrier = pltpu.get_barrier_semaphore()

    def greet(k, _):
        pl.semaphore_signal(barrier, inc=1, device_id={"sp": lax.rem(s + k, n)}, device_id_type=MESH)
        return 0

    lax.fori_loop(1, n, greet, 0)

    def greet_other(k, _):
        pl.semaphore_signal(
            barrier, inc=1, device_id={"sp": lax.rem(s + k, n), "tp": other}, device_id_type=MESH
        )
        return 0

    lax.fori_loop(0, n, greet_other, 0)
    pltpu.make_async_copy(o_in, ow, o_sem).start()

    for j in range(n // 2):
        cols = slice(j * 2 * dim, (j + 1) * 2 * dim)
        kp, vp, qp = (r[:, cols].astype(jnp.float32) for r in (k_ref, v_ref, q_ref))
        low = lax.broadcasted_iota(jnp.int32, (rows, 2 * dim), 1) < dim
        lowh = low[:half]
        top, bot = qp[:half], qp[half:]
        sbuf[2 * j, :rows, :] = jnp.where(low, kp, pltpu.roll(vp, dim, 1)).astype(jnp.bfloat16)
        sbuf[2 * j + 1, :rows, :] = jnp.where(low, pltpu.roll(kp, dim, 1), vp).astype(jnp.bfloat16)
        sbuf[2 * j, rows:, :] = jnp.where(lowh, top, pltpu.roll(bot, dim, 1)).astype(jnp.bfloat16)
        sbuf[2 * j + 1, rows:, :] = jnp.where(lowh, pltpu.roll(top, dim, 1), bot).astype(jnp.bfloat16)

    with jax.named_scope("barrier"):
        pl.semaphore_wait(barrier, 2 * n - 1)

    def qkv_copy(t, src):
        return sends(sbuf.at[t], rbuf.at[src], qkv_s.at[t], qkv_r.at[src], {"sp": t})

    def doc_copy(t, src):
        return sends(doc_ref, docr.at[src], doc_s.at[t], doc_r.at[src], {"sp": t})

    def flipped(v, k):
        bit, moved = 1, v
        while bit <= k:
            if k & bit:
                moved = moved + bit - 2 * bit * lax.rem(lax.div(moved, bit), 2)
            bit *= 2
        return moved

    for kz in NEAREST:
        for kp in range(4):
            if kz + kp > 0:
                t = flipped(s, 4 * kz + kp)
                qkv_copy(t, s).start()
                doc_copy(t, s).start()
    rbuf[pl.ds(s, 1)] = sbuf[pl.ds(s, 1)]
    docr[pl.ds(s, 1)] = doc_ref[...][None]

    mats = ((g_in, wg), (u_in, wu), (d_in, wd), (d_in, wd))
    deep = width // 2
    side = lax.div(g, per)
    sided = levels // 2
    mine = (side == c) & (y == c)

    def part_of(m, j):
        if m >= 2:
            return d_in.at[pl.ds(pl.multiple_of(j * width + (m - 2) * deep, deep), deep), :]
        return mats[m][0].at[:, pl.ds(pl.multiple_of(j * width, width), width)]

    def slot_of(m, src):
        if m >= 2:
            return wd.at[pl.ds((m - 2) * deep, deep), pl.ds(pl.multiple_of(src * dcols, dcols), dcols)]
        return mats[m][1].at[pl.ds(pl.multiple_of(src * depth, depth), depth), :]

    def w_copy(m, k):
        j = 2 * lax.rem(z + sided - lax.div(k, 2), sided) + lax.rem(y + k, 2)
        to = {"sp": 2 * (per * c + j) + x, "tp": y}
        return sends(part_of(m, j), slot_of(m, s), w_s.at[m, k], w_r.at[m, s], to)

    def own_copy(m):
        return pltpu.make_async_copy(part_of(m, lax.rem(g, per)), slot_of(m, s), own_sem.at[m])

    def parts(m):
        return (2, 3) if m == 2 else (m,)

    def start_weight(m, k):
        for e in parts(m):
            start_part(e, k)

    def start_part(m, k):
        local = mine & (k == 0)

        @pl.when(local)
        def _():
            own_copy(m).start()

        @pl.when(jnp.logical_not(local))
        def _():
            w_copy(m, k).start()

    def start_weights(m):
        for k in range(per):
            start_weight(m, k)

    def to_x(m, src, q):
        return sends(slot_of(m, src), slot_of(m, src), wx_s.at[m, q], w_r.at[m, src], {"sp": xn})

    def to_core(m, src):
        return sends(slot_of(m, src), slot_of(m, src), wc_s.at[m, src], w_r.at[m, src], {"tp": other})


    def plane(q):
        there = side if q < sided else 1 - side
        return sided * there + lax.rem(z + q, sided)

    def source(q):
        return 4 * plane(q) + 2 * c + x

    def hand_on(m, q):
        for e in parts(m):
            hand_part(e, q)

    def hand_part(m, q):
        src = source(q)
        local = mine & (src == s)

        @pl.when(local)
        def _():
            own_copy(m).wait()

        @pl.when(jnp.logical_not(local))
        def _():
            to_core(m, src).wait_recv()

        to_x(m, src, q).start()
        to_core(m, src).start()

    def pass_on(m, q):
        src = source(q) + 1 - 2 * x
        for e in parts(m):
            to_core(e, src).wait_recv()
            to_core(e, src).start()

    def arrive(m, q):
        for p in parts(m):
            for e in range(2):
                to_core(p, 4 * plane(q) + 2 * other + e).wait_recv()

    scale = dim ** (-0.5) * LOG2E
    off = off_ref[s] * LOG2E
    chunk = 2 * rows
    span = min(back, n - 1) + 1
    lane = lax.broadcasted_iota(jnp.int32, (half, 2 * dim), 1) < dim
    key_i = lax.broadcasted_iota(jnp.int32, (chunk, chunk), 0)
    key_j = lax.broadcasted_iota(jnp.int32, (chunk, chunk), 1)
    later = jnp.where(key_i > key_j, -1.0, 0.0).astype(jnp.bfloat16)
    query_i = lax.broadcasted_iota(jnp.int32, (rows, chunk), 0)
    before = lax.broadcasted_iota(jnp.int32, (rows, chunk), 1) - rows < query_i
    nt = (((1,), (1,)), ((), ()))

    def att_copy(t, src):
        return sends(ao.at[t], att_ref.at[src], att_s.at[t], att_r.at[src], {"sp": t})

    def scores(i):
        q2 = rbuf[i, rows:, :].astype(jnp.float32)
        q_pad = jnp.concatenate(
            [jnp.where(lane, q2, 0.0), jnp.where(lane, pltpu.roll(q2, dim, 1), 0.0)], axis=0
        ).astype(jnp.bfloat16)
        q_doc = jnp.broadcast_to(docr[i, 0:1, :].astype(jnp.float32), (rows, rows)).T
        q_doc = jnp.concatenate([q_doc, q_doc], axis=1)
        found = []
        for d in range(0, span, 2):
            js = [jnp.maximum(i - e, 0) for e in (d + 1, d)]
            kv = jnp.concatenate([rbuf[j, :rows, :] for j in js], axis=0)
            k_doc = jnp.concatenate(
                [
                    jnp.where(i >= e, docr[j, 0:1, :].astype(jnp.float32), -1.0)
                    for e, j in zip((d + 1, d), js)
                ],
                axis=1,
            )
            live = q_doc == k_doc
            if d == 0:
                live = live & before
            logit = lax.dot_general(q_pad, kv, nt, preferred_element_type=jnp.float32) * scale + off
            logit = jnp.where(live, logit, DEAD)
            drop = jnp.maximum(logit, 0.0) + jnp.log2(1.0 + jnp.exp2(-jnp.abs(logit)))
            found.append((logit - drop, drop.astype(jnp.bfloat16), jnp.sum(drop, axis=1, keepdims=True), kv))
        return found

    def weigh(i, found):
        carried = jnp.zeros((rows, 1), jnp.float32)
        weights = []
        for own, drop, dropped, _ in found:
            tail = jnp.dot(drop, later, preferred_element_type=jnp.float32)
            weights.append(jnp.exp2(own + (tail - carried)).astype(jnp.bfloat16))
            carried = carried + dropped
        total = jnp.dot(
            jnp.concatenate(weights, axis=1),
            jnp.concatenate([kv for _, _, _, kv in found], axis=0),
            preferred_element_type=jnp.float32,
        )
        packed = jnp.where(lane, pltpu.roll(total[:half], dim, 1), total[half:]).astype(jnp.bfloat16)

        @pl.when(i == s)
        def _():
            att_ref[pl.ds(s, 1)] = packed[None]

        @pl.when(i != s)
        def _():
            ao[pl.ds(i, 1)] = packed[None]
            att_copy(i, s).start()

    low = side == 0

    @pl.when(c == side)
    def _():
        for m in FIRST:
            start_weights(m)


    def wait_span(src, _):
        @pl.when(src != s)
        def _():
            qkv_copy(src, src).wait_recv()
            doc_copy(src, src).wait_recv()

        return 0

    def pair(t, _):
        h = jnp.where(low, t, n // 2 - 1 - t)
        deep = jnp.maximum(2 * h + 1 - span, 0)
        deep_end = jnp.where(t == 0, n, jnp.maximum(2 * h + 3 - span, 0))
        first, end = jnp.where(low, 2 * h, deep), jnp.where(low, 2 * h + 2, deep_end)
        with jax.named_scope("wait_qkv"):
            lax.fori_loop(first, end, wait_span, 0)
        with jax.named_scope("att"):
            pair_steps(t)
            found = [scores(2 * h + e) for e in range(2)]
            for e in range(2):
                weigh(2 * h + e, found[e])
        return 0

    def event(name):
        m = int(name[1])
        with jax.named_scope(name):
            if name[0] in "SIO":
                first = 0 if name[2] == "a" else per // 2
                inner = (z == sided) | (z == sided - 1)
                chosen = {"S": z >= 0, "I": inner, "O": jnp.logical_not(inner)}[name[0]]

                @pl.when((c != side) & chosen)
                def _():
                    for k in range(first, first + per // 2):
                        start_weight(m, k)
            elif name[0] == "T":
                @pl.when(c == side)
                def _():
                    start_weights(m)
            elif name[0] == "N":
                hand_on(m, int(name[2]))
            elif name[0] == "H":
                hand_on(m, sided + int(name[2]))
            elif name[0] == "P":
                pass_on(m, int(name[2]))
            elif name[0] == "A":
                arrive(m, int(name[2]))
            elif name[0] == "D":
                project_down(m, plane(int(name[2])))
            elif name[0] == "B":
                add(m, int(name[2]))
            elif name[0] == "Y":
                relay(m, True)
            elif name[0] == "R":
                relay(m, False)
            elif name[0] == "G":
                gate_up(m)

    def pair_steps(t):
        for name, at_low, at_high in LOOP:
            @pl.when(t == jnp.where(low, at_low, at_high))
            def _():
                event(name)

    with jax.named_scope("attention"):
        lax.fori_loop(0, n // 2, pair, 0)

    for name in AHEAD:
        event(name)

    def wait_attended(k, _):
        src = lax.rem(s + n - k, n)
        att_copy(src, src).wait_recv()
        return 0

    with jax.named_scope("wait_att"):
        lax.fori_loop(1, n, wait_attended, 0)
    for j in range(n // 2):
        cols = slice(j * 2 * dim, (j + 1) * 2 * dim)
        ha, hb = (att_ref[2 * j + e].astype(jnp.float32) for e in range(2))
        attd[:half, cols] = jnp.where(lane, ha, pltpu.roll(hb, dim, 1)).astype(jnp.bfloat16)
        attd[half:, cols] = jnp.where(lane, pltpu.roll(ha, dim, 1), hb).astype(jnp.bfloat16)

    pltpu.make_async_copy(o_in, ow, o_sem).wait()
    dm = ow.shape[1]
    tile = min(512, dm)

    def project(t, _):
        cols = pl.ds(pl.multiple_of(t * tile, tile), tile)
        prod = jnp.dot(attd[...], ow[:, cols], preferred_element_type=jnp.float32).astype(jnp.bfloat16)
        mixed[0, :, cols] = prod[:half]
        mixed[1, :, cols] = prod[half:]
        return 0

    with jax.named_scope("project"):
        lax.fori_loop(0, dm // tile, project, 0)
    mix = sends(mixed.at[other], mixed_in, mix_s, mix_r, {"tp": other})
    mix.start()
    with jax.named_scope("wait_mix"):
        mix.wait_recv()
    rows_f = resid_ref[...].astype(jnp.float32) + (
        mixed[c].astype(jnp.float32) + mixed_in[...].astype(jnp.float32)
    )
    stream[...] = rows_f
    inv = lax.rsqrt(jnp.mean(rows_f * rows_f, axis=1, keepdims=True) + 1e-06)
    ag[pl.ds(g, 1)] = (rows_f * inv * gain_ref[...]).astype(jnp.bfloat16)[None]

    def link(kind, k, src, dst, to):
        return sends(src, dst, net_s.at[kind, k], net_r.at[kind, k], {"sp": to})

    def up(d, zz):
        return link(0, d, ag.at[2 * zz + y], ag.at[2 * zz + y], s + 4)

    def down(d, zz):
        return link(1, d, ag.at[2 * zz + y], ag.at[2 * zz + y], s - 4)

    def across(zz):
        return link(2, zz, ag.at[2 * zz + y], ag.at[2 * zz + y], yn)

    def z_of(k):
        return flipped(z, k)

    def across_part(k, h):
        at = h * levels + k
        return link(
            3, at, part.at[2 * z_of(k) + 1 - y, :, wide(h)], fy.at[k, :, wide(h)], yn
        )

    def inward(k, h):
        at = h * levels + k
        return link(
            4, at, part.at[2 * z_of(k) + y, :, wide(h)], zr.at[k, :, wide(h)], s + 4 * (z_of(k & -k) - z)
        )

    broad = dm // levels

    def wide(h):
        return pl.ds(pl.multiple_of(h * broad, broad), broad)

    def goes_up(d):
        return (z < levels - 1) & (z - d + 1 >= 0)

    def goes_down(d):
        return (z > 0) & (z + d - 1 < levels)

    def step_up(d):
        @pl.when(goes_up(d))
        def _():
            up(d, z - d + 1).start()

    def step_down(d):
        @pl.when(goes_down(d))
        def _():
            down(d, z + d - 1).start()

    def relay(d, same):
        @pl.when((z - d >= 0) & ((lax.div(z - d + levels, sided) - 2 == side) == same))
        def _():
            up(d, z - d).wait_recv()
            across(z - d).start()
            if d + 1 < levels:
                step_up(d + 1)

        @pl.when((z + d < levels) & ((lax.div(z + d, sided) == side) == same))
        def _():
            down(d, z + d).wait_recv()
            across(z + d).start()
            if d + 1 < levels:
                step_down(d + 1)

    step_up(1)
    step_down(1)
    across(z).start()

    def gate_up(k):
        with jax.named_scope(f"wait_y{k}"):
            across(z_of(k)).wait_recv()
        with jax.named_scope(f"gate_up{k}"):
            xs = ag[pl.ds(2 * z_of(k), 2)].reshape(rows, dm)
            gate = jnp.dot(xs, wg[...], preferred_element_type=jnp.float32)
            upper = jnp.dot(xs, wu[...], preferred_element_type=jnp.float32)
            hid[k] = (gate / (1.0 + jnp.exp(-gate)) * upper).astype(jnp.bfloat16)

    def project_down(k, h):
        prod = jnp.dot(hid[k], wd[:, wide(h)], preferred_element_type=jnp.float32)
        part[pl.ds(2 * z_of(k), 2), :, wide(h)] = prod.astype(jnp.bfloat16).reshape(2, half, broad)
        across_part(k, h).start()

    def direct(h):
        far = z_of(levels - 1)
        return link(4, h * levels, part.at[2 * far + y, :, wide(h)], zr.at[0, :, wide(h)], s + 4 * (far - z))

    def outward(k, q):
        h = plane(q)
        return direct(h) if k == q == levels - 1 else inward(k, h)

    def add(k, q):
        h = plane(q)
        across_part(k, h).wait_recv()
        at = 2 * z_of(k) + y
        summed = part[at, :, wide(h)].astype(jnp.float32) + fy[k, :, wide(h)].astype(jnp.float32)
        if k == 0:
            stream[:, wide(h)] = stream[:, wide(h)] + summed
        else:
            if k == levels - 2 and q != levels - 2:
                inward(k + 1, h).wait_recv()
                summed = summed + zr[k + 1, :, wide(h)].astype(jnp.float32)
            part[at, :, wide(h)] = summed.astype(jnp.bfloat16)
            outward(k, q).start()

    for name in AFTER:
        event(name)
    with jax.named_scope("last"):
        for q in range(levels):
            h = plane(q)
            summed = stream[:, wide(h)]
            for j in range(1, levels):
                if j == j & -j:
                    inward(j, h).wait_recv()
                    summed = summed + zr[j, :, wide(h)].astype(jnp.float32)
            if q == 0:
                direct(h).wait_recv()
                summed = summed + zr[0, :, wide(h)].astype(jnp.float32)
            out_ref[:, wide(h)] = summed.astype(jnp.bfloat16)

    with jax.named_scope("finish"):
        mix.wait_send()
        for k in range(levels):
            across(k).wait_send()
            for q in range(levels):
                across_part(k, plane(q)).wait_send()
                if k > 0:
                    outward(k, q).wait_send()
            if k > 0:
                @pl.when(goes_up(k))
                def _():
                    up(k, z - k + 1).wait_send()

                @pl.when(goes_down(k))
                def _():
                    down(k, z + k - 1).wait_send()

        def finish_peer(k, _):
            src = lax.rem(s + n - k, n)
            att_copy(src, src).wait_send()
            qkv_copy(src, src).wait_send()
            doc_copy(src, src).wait_send()
            return 0

        lax.fori_loop(1, n, finish_peer, 0)
        for m in range(len(mats)):
            for q in range(levels):
                to_x(m, source(q), q).wait_send()
                to_core(m, source(q)).wait_send()
                to_core(m, source(q) + 1 - 2 * x).wait_send()

            @pl.when(jnp.logical_not(mine))
            def _():
                w_copy(m, 0).wait_send()

            for k in range(1, per):
                w_copy(m, k).wait_send()


def resharded(
    resid, queries, keys, values, doc_ids, score_offset, out_weight, norm_gain,
    gate_weight, up_weight, down_weight,
):
    n, ntp = lax.axis_size("sp"), lax.axis_size("tp")
    rows, local = queries.shape
    half, two = rows // 2, 2 * (local // n)
    dm = resid.shape[1]
    groups, levels = n // 2, n // 4
    width = gate_weight.shape[1] * ntp // groups
    per = groups // ntp
    bf, f32 = jnp.bfloat16, jnp.float32
    vmem = pl.BlockSpec(memory_space=pltpu.VMEM)
    anyw = pl.BlockSpec(memory_space=pl.ANY)
    dma = pltpu.SemaphoreType.DMA
    block = (half, dm)
    return pl.pallas_call(
        functools.partial(layer_kernel, n),
        out_shape=jax.ShapeDtypeStruct(block, bf),
        in_specs=[vmem] * 4 + [pl.BlockSpec(memory_space=pltpu.SMEM)] + [anyw] * 3 + [vmem] * 2 + [anyw],
        out_specs=vmem,
        scratch_shapes=[
            pltpu.VMEM((n, rows + half, two), bf),
            pltpu.VMEM((n, rows + half, two), bf),
            pltpu.VMEM((n, 1, rows), jnp.int32),
            pltpu.VMEM((n, half, two), bf),
            pltpu.VMEM((n, half, two), bf),
            pltpu.VMEM((dm, width), bf),
            pltpu.VMEM((dm, width), bf),
            pltpu.VMEM((width, dm), bf),
            pltpu.VMEM(out_weight.shape, bf),
            pltpu.VMEM((rows, local), bf),
            pltpu.VMEM((2,) + block, bf),
            pltpu.VMEM(block, bf),
            pltpu.VMEM(block, f32),
            pltpu.VMEM((groups,) + block, bf),
            pltpu.VMEM((levels, rows, width), bf),
            pltpu.VMEM((groups,) + block, bf),
            pltpu.VMEM((levels,) + block, bf),
            pltpu.VMEM((levels,) + block, bf),
            dma((n,)), dma((n,)), dma((n,)), dma((n,)), dma((n,)), dma((n,)),
            dma((4, per)), dma((4, n)), dma((4, levels)), dma((4, n)), dma((4,)),
            dma, dma, dma, dma((5, levels * levels)), dma((5, levels * levels)),
        ],
        compiler_params=pltpu.CompilerParams(has_side_effects=True, collective_id=0, vmem_limit_bytes=60 << 20),
    )(
        queries, keys, values, doc_ids[None], score_offset,
        gate_weight, up_weight, down_weight, resid, norm_gain[None], out_weight,
    )


def on_device(*args):
    queries, doc_ids, score_offset, gate_weight = args[1], args[4], args[5], args[8]
    n, ntp = lax.axis_size("sp"), lax.axis_size("tp")
    dim = queries.shape[1] // score_offset.shape[0]
    fits = (
        ntp == 2
        and n == 4 * len(NEAREST)
        and score_offset.shape[0] == n
        and 2 * dim == 128
        and doc_ids.shape[0] == 128
        and gate_weight.shape[1] * ntp % (n * 64) == 0
        and gate_weight.shape[0] % 128 == 0
    )
    return resharded(*args) if fits else windowed(*args)


def solution(mesh):
    in_specs = (
        P(("sp", "tp"), None),
        P("sp", "tp"),
        P("sp", "tp"),
        P("sp", "tp"),
        P("sp"),
        P("tp"),
        P("tp", None),
        P(),
        P("sp", "tp"),
        P("sp", "tp"),
        P("tp", "sp"),
    )
    out_specs = P(("sp", "tp"), None)
    return jax.shard_map(
        on_device, mesh=mesh, in_specs=in_specs, out_specs=out_specs, check_vma=False
    )
```
